32 devices in a mesh: ep: 8 (over z, x), tp: 4 (over y, core).
Axes of the slice: x: 2, y: 2, z: 4, core: 2. Of those that a mesh axis runs over, the one named last changes fastest.
Arguments:
- query_rows: bfloat16 [3072, 1024], P('ep', 'tp'), may hold values from -8 to 8
- key_rows: bfloat16 [3072, 256], P('ep'), may hold values from -8 to 8
- value_rows: bfloat16 [3072, 256], P('ep'), may hold values from -6 to 6
- query_gain: float32 [64], replicated, may hold values from 0.3 to 6
- key_gain: float32 [64], replicated, may hold values from 0.3 to 6
- out_weight: bfloat16 [1024, 2048], P('tp'), may hold values from -0.1875 to 0.1875
- mixer_gain: float32 [2048], replicated, may hold values from 0.1 to 1.9
- expert_input: bfloat16 [2048, 2048], P('ep'), may hold values from -6 to 6
- expert_ids: int32 [2048, 2], P('ep'), may hold values from 0 to 7, all different within a row; in each aligned block of 256 rows (0 to 255, 256 to 511, ...) at most 96 rows name the same one
- gate_score: float32 [2048, 2], P('ep'), may hold values from 0.05 to 1
- expert_gain: float32 [2048], replicated, may hold values from 0.1 to 1.9
- gate_weight: bfloat16 [8, 2048, 4096], P('ep', None, 'tp'), may hold values from -0.125 to 0.125
- up_weight: bfloat16 [8, 2048, 4096], P('ep', None, 'tp'), may hold values from -0.125 to 0.125
- down_weight: bfloat16 [8, 4096, 2048], P('ep', 'tp'), may hold values from -0.09375 to 0.09375
- shared_gate: bfloat16 [2048, 2048], P(None, 'tp'), may hold values from -0.125 to 0.125
- shared_up: bfloat16 [2048, 2048], P(None, 'tp'), may hold values from -0.125 to 0.125
- shared_down: bfloat16 [2048, 2048], P('tp'), may hold values from -0.125 to 0.125
Outputs:
- mixer_out: bfloat16 [3072, 2048], P('ep')
- expert_out: bfloat16 [2048, 2048], P('ep', 'tp')
The draws below stay inside these ranges and needn't reach their ends.
Inputs may be any that keep to these rules, and one draw needn't show every extreme that they name: `expert_ids`: each row names 2 different experts. In each aligned block of 256 rows (the rows of one device) no expert is named by more than 96 rows, a bound that some block reaches.
All inputs are finite; a program needn't handle non-finite values.
Results may differ from the reference program's by a relative error of at most 0.02.
The reference program's roundings to bfloat16 on the way count: a program that leaves them out, or rounds other values in their place, can miss the bound.
Values may be sent and summed in bfloat16 or wider, within the bound.
A program may use at most 128 MiB of HBM per device.

```python
import math
import jax
import jax.numpy as jnp
import numpy as np
from jax import lax

D = 2048
HEADS = 16
KV_HEADS = 4
HEAD_DIM = 64
GRID_W = 64
EXPERT_DIM = 4096
SHARED_DIM = 2048
TOP = 2
RA = 384
RB = 256
TA = 3072
TB = 2048
EXPERTS = 8
CAP = 96
N_EP = 8
N_TP = 4


def draw_query_rows(key, part):
    drawn = jax.random.normal(jax.random.fold_in(key, 11), (TA, HEADS * HEAD_DIM), jnp.float32)
    drawn = jnp.clip(drawn, -6.0, 6.0)
    return drawn.astype(jnp.bfloat16)


def draw_key_rows(key, part):
    drawn = jax.random.normal(jax.random.fold_in(key, 12), (TA, KV_HEADS * HEAD_DIM), jnp.float32)
    drawn = jnp.clip(drawn, -6.0, 6.0)
    return drawn.astype(jnp.bfloat16)


def gain_draw(key, salt):
    drawn = 1.0 + 0.18 * jax.random.normal(jax.random.fold_in(key, salt), (HEAD_DIM,), jnp.float32)
    drawn = jnp.clip(drawn, 0.3, 1.7)
    return drawn.astype(jnp.float32)


def draw_query_gain(key, part):
    return gain_draw(key, 21)


def draw_key_gain(key, part):
    return gain_draw(key, 22)


def shard_levels(key, shape, cuts, low, top_value):
    level, own = 1.0, jax.random.fold_in(key, 6)
    for dim, parts in cuts:
        heights = jnp.exp(jax.random.uniform(jax.random.fold_in(own, dim), (parts,), jnp.float32, low / len(cuts), top_value / len(cuts)))
        level = level * jnp.repeat(heights, shape[dim] // parts).reshape([-1 if axis == dim else 1 for axis in range(len(shape))])
    return level


def assign_block(rng, own, number, rows, count, top, limit, lean):
    sequence = jax.random.permutation(rng, count)
    heavy_load, ordinary = load_shares(count, rows * top, limit, lean, True), load_shares(count, rows * top, limit, lean, False)
    places = jnp.arange(count)

    def named(tallies, rotation):
        used = int((tallies > 0).sum())
        fixed = max(1, used // 4)
        moved = fixed + (places - fixed + rotation * (used - fixed)) % max(1, count - fixed)
        return jnp.zeros((count,), jnp.int32).at[sequence[jnp.where(places < fixed, places, moved)]].set(jnp.asarray(tallies, jnp.int32))

    tallies = jnp.where(number % 4 == 0, named(heavy_load, number // 4), named(ordinary, number - number // 4 - 1))
    mixed = jax.random.permutation(jax.random.fold_in(own, 3), count)
    donor, taker = mixed[0:count // 2 * 2:2], mixed[1:count // 2 * 2:2]
    slack = jnp.minimum(tallies[donor] - 1, limit - tallies[taker]) // 2
    slack = jnp.where((donor == sequence[0]) | (taker == sequence[0]) | (tallies[taker] == 0), 0, jnp.maximum(slack, 0))
    moved = jax.random.randint(jax.random.fold_in(own, 4), (count // 2,), 0, 1 << 20) % (slack + 1)
    tallies = tallies.at[donor].add(-moved).at[taker].add(moved)
    items = jnp.searchsorted(jnp.cumsum(tallies), jnp.arange(rows * top), side="right").astype(jnp.int32)
    table = items.reshape(top, rows).T
    table = table[jax.random.permutation(jax.random.fold_in(own, 1), rows)]
    rotation = jax.random.randint(jax.random.fold_in(own, 2), (rows, 1), 0, top)
    return jnp.take_along_axis(table, (jnp.arange(top)[None, :] + rotation) % top, axis=1)


def load_shares(number_of, total, bound, lean, full):
    weights = [(1 << 20) // math.isqrt(standing ** lean) + 1 for standing in range(1, number_of + 1)]
    largest = bound if full else min(bound, max(-(-total // number_of), total * weights[0] // sum(weights)))
    least = 1 if total - largest >= number_of - 1 else 0
    holding, spare = [largest] + [least] * (number_of - 1), total - largest - least * (number_of - 1)
    while spare > 0:
        free = [i for i in range(1, number_of) if holding[i] < largest] or [i for i in range(1, number_of) if holding[i] < bound]
        pool, budget = sum([weights[i] for i in free]), spare
        for i in free:
            addition = min(bound - holding[i], max(1, budget * weights[i] // pool), spare)
            holding[i] = holding[i] + addition
            spare = spare - addition
    return np.array(holding)


def centred(own_key, extent, spread, most, pieces=(), kind=jnp.bfloat16):
    result = spread * jax.random.normal(own_key, extent, jnp.float32)
    if pieces:
        result = result * shard_levels(own_key, extent, pieces, -0.22, 0.18)
    return jnp.clip(result, -most, most).astype(kind)


def setup_inputs(seed: int = 0) -> dict:
    key_of = jax.random.split(jax.random.key(seed), 18)
    query_rows = draw_query_rows(jax.random.fold_in(key_of[17], 71), 0)
    key_rows = draw_key_rows(jax.random.fold_in(key_of[17], 71), 0)
    value_rows = centred(key_of[2], (TA, KV_HEADS * HEAD_DIM), 1.0, 6.0, ((0, 8),))
    query_gain = draw_query_gain(jax.random.fold_in(key_of[17], 71), 0)
    key_gain = draw_key_gain(jax.random.fold_in(key_of[17], 71), 0)
    out_weight = centred(key_of[5], (HEADS * HEAD_DIM, D), (HEADS * HEAD_DIM) ** -0.5, 0.1875, ((0, 4),))
    mixer_gain = jnp.clip(1.0 + 0.18 * jax.random.normal(key_of[6], (D,), jnp.float32), 0.1, 1.9)
    expert_input = centred(key_of[7], (TB, D), 1.0, 6.0, ((0, 8),))
    expert_ids_keys = jax.random.split(jax.random.fold_in(key_of[8], 1), TB // RB)
    expert_ids_turns = jax.random.permutation(jax.random.fold_in(key_of[8], 3), TB // RB)
    expert_ids = jax.vmap(lambda own, number: assign_block(jax.random.fold_in(key_of[8], 2), own, number, RB, EXPERTS, TOP, CAP, 2))(expert_ids_keys, expert_ids_turns).reshape((TB, TOP))
    gate_score = jnp.clip(jnp.exp(math.log(1.0) - 2.9957323 * jax.random.uniform(key_of[9], (TB, TOP), jnp.float32) ** shard_levels(key_of[9], (TB, TOP), ((0, 8),), -0.2, 0.2)), 0.05, 1.0)
    expert_gain = jnp.clip(1.0 + 0.18 * jax.random.normal(key_of[10], (D,), jnp.float32), 0.1, 1.9)
    gate_weight = centred(key_of[11], (EXPERTS, D, EXPERT_DIM), D ** -0.5, 0.125, ((0, 8), (2, 4)))
    up_weight = centred(key_of[12], (EXPERTS, D, EXPERT_DIM), D ** -0.5, 0.125, ((0, 8), (2, 4)))
    down_weight = centred(key_of[13], (EXPERTS, EXPERT_DIM, D), EXPERT_DIM ** -0.5, 0.09375, ((0, 8), (1, 4)))
    shared_gate = centred(key_of[14], (D, SHARED_DIM), D ** -0.5, 0.125, ((1, 4),))
    shared_up = centred(key_of[15], (D, SHARED_DIM), D ** -0.5, 0.125, ((1, 4),))
    shared_down = centred(key_of[16], (SHARED_DIM, D), SHARED_DIM ** -0.5, 0.125, ((0, 4),))
    return {"query_rows": query_rows, "key_rows": key_rows, "value_rows": value_rows, "query_gain": query_gain, "key_gain": key_gain, "out_weight": out_weight, "mixer_gain": mixer_gain, "expert_input": expert_input, "expert_ids": expert_ids, "gate_score": gate_score, "expert_gain": expert_gain, "gate_weight": gate_weight, "up_weight": up_weight, "down_weight": down_weight, "shared_gate": shared_gate, "shared_up": shared_up, "shared_down": shared_down}


EPSILON = 1e-06
ROUTED_SCALE = 2.5

def rotary_angles(position):
    grid_row = (position // GRID_W).astype(jnp.float32)
    grid_col = (position % GRID_W).astype(jnp.float32)
    quarter = HEAD_DIM // 4
    inverse = 10000.0 ** (-jnp.arange(quarter, dtype=jnp.float32) / quarter)
    return jnp.concatenate([grid_row[:, None] * inverse, grid_col[:, None] * inverse], axis=1)

def normalize_rotate(heads_in, gain_vector, angles):
    widened = heads_in.astype(jnp.float32)
    scaled = widened * lax.rsqrt(lax.optimization_barrier(jnp.mean(widened * widened, axis=-1, keepdims=True)) + EPSILON)
    scaled = scaled * gain_vector.astype(jnp.float32)
    half_dim = scaled.shape[-1] // 2
    front_half = scaled[..., :half_dim]
    back_half = scaled[..., half_dim:]
    cosine_table = jnp.cos(angles)[:, None, :]
    sine_table = jnp.sin(angles)[:, None, :]
    turned = jnp.concatenate([front_half * cosine_table - back_half * sine_table, front_half * sine_table + back_half * cosine_table], axis=-1)
    return turned.astype(jnp.bfloat16)

def swiglu(rows_in, gate_matrix, up_matrix):
    gate_value = jnp.dot(rows_in, gate_matrix, preferred_element_type=jnp.float32)
    up_value = jnp.dot(rows_in, up_matrix, preferred_element_type=jnp.float32)
    return (jax.nn.silu(gate_value) * up_value).astype(jnp.bfloat16)

def lane_sum(hidden, down_matrix):
    group_units = hidden.shape[1] // N_TP

    def add_group(carry, group_index):
        part_hidden = lax.dynamic_slice_in_dim(hidden, group_index * group_units, group_units, 1)
        part_down = lax.dynamic_slice_in_dim(down_matrix, group_index * group_units, group_units, 0)
        partial_value = jnp.dot(part_hidden, part_down, preferred_element_type=jnp.float32).astype(jnp.bfloat16)
        return (carry + lax.optimization_barrier(partial_value).astype(jnp.float32), None)
    start_total = jnp.zeros((hidden.shape[0], down_matrix.shape[1]), jnp.float32)
    total, unused = lax.scan(add_group, start_total, jnp.arange(N_TP, dtype=jnp.int32))
    return total

def fill_slots(empty_table, slot_rows, row_numbers):
    return empty_table.at[slot_rows].set(row_numbers)

def reference(query_rows, key_rows, value_rows, query_gain, key_gain, out_weight, mixer_gain, expert_input, expert_ids, gate_score, expert_gain, gate_weight, up_weight, down_weight, shared_gate, shared_up, shared_down):
    group = HEADS // KV_HEADS
    angles = rotary_angles(jnp.arange(TA, dtype=jnp.int32))
    query_rot = normalize_rotate(query_rows.reshape(TA, HEADS, HEAD_DIM), query_gain, angles)
    key_rot = normalize_rotate(key_rows.reshape(TA, KV_HEADS, HEAD_DIM), key_gain, angles)
    value_heads = value_rows.reshape(TA, KV_HEADS, HEAD_DIM)
    scale_factor = HEAD_DIM ** (-0.5)
    block_count = TA // RA

    def one_head(head_index):
        kv_index = head_index // group
        head_keys = lax.dynamic_index_in_dim(key_rot, kv_index, 1, keepdims=False)
        head_values = lax.dynamic_index_in_dim(value_heads, kv_index, 1, keepdims=False)
        head_queries = lax.dynamic_index_in_dim(query_rot, head_index, 1, keepdims=False)

        def one_block(query_block):
            scores = jnp.dot(query_block, head_keys.T, preferred_element_type=jnp.float32) * scale_factor
            row_peak = lax.optimization_barrier(jnp.max(scores, axis=1, keepdims=True))
            exponent = jnp.exp(scores - row_peak)
            row_total = lax.optimization_barrier(jnp.sum(exponent, axis=1, keepdims=True))
            weighted = jnp.dot(exponent.astype(jnp.bfloat16), head_values, preferred_element_type=jnp.float32)
            return (weighted / row_total).astype(jnp.bfloat16)
        return lax.map(one_block, head_queries.reshape(block_count, RA, HEAD_DIM)).reshape(TA, HEAD_DIM)
    attended = lax.map(one_head, jnp.arange(HEADS, dtype=jnp.int32))
    lane_heads = HEADS // N_TP
    attended_lanes = attended.reshape(N_TP, lane_heads, TA, HEAD_DIM)
    weight_lanes = out_weight.reshape(N_TP, lane_heads, HEAD_DIM, D)

    def add_lane(carry, packed):
        lane_attended, lane_weight = packed
        partial_value = jnp.einsum('hqd,hde->qe', lane_attended.astype(jnp.float32), lane_weight.astype(jnp.float32))
        rounded = lax.optimization_barrier(partial_value.astype(jnp.bfloat16))
        return (carry + rounded.astype(jnp.float32), None)
    mixer_sum, unused = lax.scan(add_lane, jnp.zeros((TA, D), jnp.float32), (attended_lanes, weight_lanes))
    mixer_scale = lax.rsqrt(lax.optimization_barrier(jnp.mean(mixer_sum * mixer_sum, axis=1, keepdims=True)) + EPSILON)
    mixer_out = (mixer_sum * mixer_scale * mixer_gain.astype(jnp.float32)).astype(jnp.bfloat16)
    widened = expert_input.astype(jnp.float32)
    normed = (widened * lax.rsqrt(lax.optimization_barrier(jnp.mean(widened * widened, axis=1, keepdims=True)) + EPSILON) * expert_gain.astype(jnp.float32)).astype(jnp.bfloat16)
    route_weight = gate_score / lax.optimization_barrier(jnp.sum(gate_score, axis=1, keepdims=True)) * ROUTED_SCALE
    pair_ids = expert_ids.reshape(N_EP, RB * TOP)
    onehot = (pair_ids[:, :, None] == jnp.arange(EXPERTS, dtype=jnp.int32)).astype(jnp.int32)
    ranks = lax.optimization_barrier(jnp.sum((jnp.cumsum(onehot, axis=1, dtype=jnp.int32) - 1) * onehot, axis=2, dtype=jnp.int32))
    slot_index = (pair_ids * CAP + ranks).astype(jnp.int32)
    row_numbers = (jnp.arange(N_EP, dtype=jnp.int32)[:, None] * RB + jnp.arange(RB * TOP, dtype=jnp.int32)[None, :] // TOP).astype(jnp.int32)
    sources = jnp.full((N_EP, EXPERTS * CAP), -1, jnp.int32)
    sources = jax.vmap(fill_slots)(sources, slot_index, row_numbers)
    expert_sources = sources.reshape(N_EP, EXPERTS, CAP).transpose(1, 0, 2).reshape(EXPERTS, N_EP * CAP)

    def one_expert(packed):
        source_rows, gate_matrix, up_matrix, down_matrix = packed
        filled = (source_rows >= 0)[:, None]
        picked = jnp.where(filled, normed[jnp.maximum(source_rows, 0)], jnp.zeros((), jnp.bfloat16))
        hidden = swiglu(picked, gate_matrix, up_matrix)
        return lane_sum(hidden, down_matrix).astype(jnp.bfloat16)
    expert_result = lax.map(one_expert, (expert_sources, gate_weight, up_weight, down_weight))
    flat_result = expert_result.reshape(EXPERTS * N_EP * CAP, D)
    block_of = (jnp.arange(TB, dtype=jnp.int32) // RB)[:, None]
    result_index = (expert_ids * (N_EP * CAP) + block_of * CAP + ranks.reshape(TB, TOP)).astype(jnp.int32)
    picked_results = flat_result[result_index]
    routed = lax.optimization_barrier(jnp.sum(picked_results.astype(jnp.float32) * route_weight[:, :, None], axis=1))
    shared_hidden = swiglu(normed, shared_gate, shared_up)
    shared_sum = lane_sum(shared_hidden, shared_down)
    expert_out = (routed + shared_sum).astype(jnp.bfloat16)
    return (mixer_out, expert_out)
```

```python
import functools

import jax
import jax.numpy as jnp
from jax import lax
from jax.experimental import pallas as pl
from jax.experimental.pallas import tpu as pltpu
from jax.sharding import PartitionSpec as P

HEADS = 16
KV_HEADS = 4
HEAD_DIM = 64
GRID_W = 64

EPSILON = 1e-06
ROUTED_SCALE = 2.5
F32 = jnp.float32
BF16 = jnp.bfloat16
MESH = pl.DeviceIdType.MESH


def rotary_angles(position):
    grid_row = (position // GRID_W).astype(F32)
    grid_col = (position % GRID_W).astype(F32)
    quarter = HEAD_DIM // 4
    inverse = 10000.0 ** (-jnp.arange(quarter, dtype=F32) / quarter)
    return jnp.concatenate([grid_row[:, None] * inverse, grid_col[:, None] * inverse], axis=1)


def normalize_rotate(heads_in, gain_vector, angles):
    widened = heads_in.astype(F32)
    scaled = widened * lax.rsqrt(jnp.mean(widened * widened, axis=-1, keepdims=True) + EPSILON)
    scaled = scaled * gain_vector
    half_dim = scaled.shape[-1] // 2
    front_half = scaled[..., :half_dim]
    back_half = scaled[..., half_dim:]
    cosine_table = jnp.cos(angles)[:, None, :]
    sine_table = jnp.sin(angles)[:, None, :]
    turned = jnp.concatenate(
        [
            front_half * cosine_table - back_half * sine_table,
            front_half * sine_table + back_half * cosine_table,
        ],
        axis=-1,
    )
    return turned.astype(BF16)


def silu(v):
    return v / (1.0 + jnp.exp(-v))


def dot(a, b):
    return jnp.dot(a, b, preferred_element_type=F32)


def fused_kernel(
    sizes,
    kv_in, out_in, q_in, normed_in, pick_in, gain_in,
    sg_hbm, su_hbm, sd_hbm, ow_hbm, wg_hbm, wu_hbm, wd_hbm,
    mixer_ref, expert_ref,
    sg, su, sd, ow, wg, wu, wd,
    kv, att, mp, mrecv, msum, my, mo, xh, hid, po, rp, tt, yr, fin, ret,
    sho, shs, shr, shp, shv,
    w_sem, kv_s, kv_r, kf_s, d_s, d_r, m_s, m_r, g_s, g_r, sh_sem, v_s, v_r, mp_sem, my_s, my_r, mo_sem,
    p_s, p_r, u_s, u_r, r_s, r_r,
):
    n, tp_n, ny, heads, cp, lc, xs = sizes
    zs = n // xs
    me = lax.axis_index("ep")
    tp = lax.axis_index("tp")
    core = tp % 2
    y = tp // 2
    mate = tp + 1 - 2 * core
    other = 1 - core
    my_z = me // xs
    my_x = me % xs
    ra = kv_in.shape[0]
    half = ra // 2

    def send(src, dst, ssem, rsem, ep=None, t=None):
        return pltpu.make_async_remote_copy(
            src_ref=src, dst_ref=dst, send_sem=ssem, recv_sem=rsem,
            device_id=(me if ep is None else ep, tp if t is None else t), device_id_type=MESH,
        )

    def rows(block, size):
        return pl.ds(pl.multiple_of(block * size, size), size)

    def each(lo, hi, fn):
        def step(i, c):
            fn(i)
            return c
        lax.fori_loop(lo, hi, step, 0)

    weights = [
        pltpu.make_async_copy(a, b, w_sem.at[i])
        for i, (a, b) in enumerate(
            ((sg_hbm, sg), (su_hbm, su), (sd_hbm, sd), (ow_hbm, ow), (wg_hbm, wg), (wu_hbm, wu), (wd_hbm, wd))
        )
    ]
    for copy in weights:
        copy.start()

    barrier = pltpu.get_barrier_semaphore()

    def greet(s):
        pl.semaphore_signal(barrier, inc=1, device_id=((me + s) % n, tp), device_id_type=MESH)

    def greet_y(s):
        pl.semaphore_signal(barrier, inc=1, device_id=(me, (tp + 2 * s) % tp_n), device_id_type=MESH)

    each(1, n, greet)
    each(1, ny, greet_y)
    pl.semaphore_signal(barrier, inc=1, device_id=(me, mate), device_id_type=MESH)
    pl.semaphore_wait(barrier, n - 1 + ny - 1 + 1)

    def kv_copy(src, to):
        return send(kv_in, kv.at[rows(src, ra)], kv_s.at[to], kv_r.at[src], ep=to)

    def kv_forward(src_z, s):
        src = src_z * xs + my_x
        x_to = (my_x + s) % xs
        return send(
            kv.at[rows(src, ra)], kv.at[rows(src, ra)], kf_s.at[src_z * xs + x_to], kv_r.at[src], ep=my_z * xs + x_to)

    def z_peer(s):
        return ((my_z + s) % zs) * xs + my_x

    def x_peer(s):
        return my_z * xs + (my_x + s) % xs

    each(1, zs, lambda s: kv_copy(me, z_peer(s)).start())
    each(1, xs, lambda s: kv_copy(me, x_peer(s)).start())

    def d_copy(src, to):
        return send(out_in.at[rows(to, cp)], xh.at[tp, rows(src, cp)], d_s.at[to], d_r.at[src], ep=to)

    def m_copy(q, src):
        block = xh.at[2 * q + core, rows(src, cp)]
        return send(block, block, m_s.at[q, src], m_r.at[q, src], t=mate)

    def m_arrive(q, src):
        block = xh.at[2 * q + other, rows(src, cp)]
        return send(block, block, m_s.at[q, src], m_r.at[q, src], t=mate)

    def g_copy(by, q, src):
        block = xh.at[2 * by + core, rows(src, cp)]
        return send(block, block, g_s.at[q, src], g_r.at[by, src], t=2 * q + core)

    each(1, n, lambda s: d_copy(me, (me + s) % n).start())

    own_block = out_in.at[rows(me, cp)]
    own_place = xh.at[tp, rows(me, cp)]
    own_mate = send(own_block, own_place, m_s.at[y, me], m_r.at[y, me], t=mate)

    def own_y(s):
        q = (y + s) % ny
        return send(own_block, own_place, g_s.at[q, me], g_r.at[y, me], t=2 * q + core)

    own_mate.start()
    each(1, ny, lambda s: own_y(s).start())
    kv[rows(me, ra), :] = kv_in[...]
    xh[tp, rows(me, cp), :] = out_in[rows(me, cp), :]

    for i in range(2):
        weights[i].wait()
    normed = normed_in[...]
    sh_hidden = (silu(dot(normed, sg[...])) * dot(normed, su[...])).astype(BF16)

    def kv_pass(s):
        src_z = (my_z + zs - s) % zs
        kv_copy(src_z * xs + my_x, me).wait_recv()
        each(1, xs, lambda t: kv_forward(src_z, t).start())

    each(1, zs, kv_pass)

    def cols(tile):
        return pl.ds(pl.multiple_of(tile * lc, lc), lc)

    weights[2].wait()
    for q in range(ny):
        sho[q] = dot(sh_hidden, sd[:, cols(2 * q + other)]).astype(BF16)
    sh_copy = send(sho, shr, sh_sem.at[0], sh_sem.at[1], t=mate)
    sh_copy.start()
    for q in range(ny):
        shs[q] = dot(sh_hidden, sd[:, cols(2 * q + core)]).astype(BF16)

    def v_copy(by, q):
        return send(shp.at[q], shv.at[by], v_s.at[q], v_r.at[by], t=2 * q + core)

    sh_copy.wait_recv()
    each(0, ny, lambda q: shp.__setitem__(q, (shs[q].astype(F32) + shr[q].astype(F32)).astype(BF16)))
    each(1, ny, lambda s: v_copy(y, (y + s) % ny).start())

    def kv_rest(s):
        x_from = (my_x + xs - s) % xs
        each(0, zs, lambda t: kv_copy(((my_z + t) % zs) * xs + x_from, me).wait_recv())

    each(1, xs, kv_rest)

    def pass_on(s):
        src = (me + n - s) % n
        d_copy(src, me).wait_recv()
        m_copy(y, src).start()
        each(1, ny, lambda t: g_copy(y, (y + t) % ny, src).start())

    def pass_y(s):
        src = (me + n - s) % n

        def one(t):
            q = (y + t) % ny
            g_copy(q, y, src).wait_recv()
            m_copy(q, src).start()

        each(1, ny, one)

    total = kv.shape[0]
    bq = max(16, min(ra, 128 * 3072 // total // 16 * 16))
    while ra % bq:
        bq -= 16
    per_head = ra // bq

    def attend(i):
        block = q_in[pl.ds(pl.multiple_of(i * bq, bq), bq), :]
        scores = lax.dot_general(block, kv[...], (((1,), (1,)), ((), ())), preferred_element_type=F32)
        peak = jnp.max(scores, axis=1, keepdims=True)
        exponent = jnp.exp(scores - peak)
        row_total = jnp.sum(exponent, axis=1, keepdims=True)
        weighted = dot(exponent.astype(BF16), kv[...])
        att[pl.ds(pl.multiple_of((i % per_head) * bq, bq), bq),
            pl.ds(pl.multiple_of((i // per_head) * 128, 128), 128)] = (weighted / row_total).astype(BF16)

    steps = heads * per_head
    pair = 2 if steps % 2 == 0 else 1
    turns = steps // pair

    def attend_pair(i):
        for j in range(pair):
            attend(i * pair + j)
        lo = 1 + i * (n - 1) // turns
        hi = 1 + (i + 1) * (n - 1) // turns

        def step(s):
            pass_on(s)
            pass_y(s - 1)

        each(lo, hi, step)

    each(0, turns, attend_pair)
    pass_y(n - 1)

    weights[3].wait()
    width = mp.shape[1]
    tile = min(512, width)

    def project(t):
        at = pl.ds(pl.multiple_of(t * tile, tile), tile)
        mp[:, at] = dot(att[...], ow[:, at]).astype(BF16)

    each(0, width // tile, project)
    mp_copy = send(mp.at[rows(other, half)], mrecv, mp_sem.at[0], mp_sem.at[1], t=mate)
    mp_copy.start()

    weights[4].wait()
    weights[5].wait()
    each(0, n, lambda s: each(0, ny, lambda q: m_arrive(q, s).wait_recv()))
    ft = min(256, hid.shape[1])

    def gate_up(t):
        at = pl.ds(pl.multiple_of(t * ft, ft), ft)
        gate = dot(xh[0], wg[0:lc, at])
        up = dot(xh[0], wu[0:lc, at])
        for j in range(1, tp_n):
            gate = gate + dot(xh[j], wg[j * lc:(j + 1) * lc, at])
            up = up + dot(xh[j], wu[j * lc:(j + 1) * lc, at])
        hid[:, at] = (silu(gate) * up).astype(BF16)

    each(0, 1, gate_up)
    mp_copy.wait_recv()
    msum[...] = (mp[rows(core, half), :].astype(F32) + mrecv[...].astype(F32)).astype(BF16)

    def my_copy(src, to):
        return send(msum, my.at[src], my_s.at[to], my_r.at[src], t=2 * to + core)

    each(1, ny, lambda s: my_copy(y, (y + s) % ny).start())
    my[y] = msum[...]
    each(1, hid.shape[1] // ft, gate_up)

    weights[6].wait()
    hn = n // 2
    hs = hn * cp
    near = me // hn
    far = 1 - near

    def p_copy(hf, q):
        return send(po.at[q, rows(hf, hs)], rp.at[q, rows(hf, hs)], p_s.at[hf, q], p_r.at[hf, q], t=mate)

    def down_other(hf, q):
        po[q, rows(hf, hs), :] = dot(hid[rows(hf, hs), :], wd[:, cols(2 * q + other)]).astype(BF16)
        p_copy(hf, q).start()

    def u_copy(by, q, to):
        return send(tt.at[q, rows(to, cp)], yr.at[by, rows(to, cp)], u_s.at[q, to], u_r.at[by, to], t=2 * q + core)

    def down_own(hf, q):
        own = dot(hid[rows(hf, hs), :], wd[:, cols(2 * q + core)]).astype(BF16).astype(F32)
        p_copy(hf, q).wait_recv()
        tt[q, rows(hf, hs), :] = (own + rp[q, rows(hf, hs), :].astype(F32)).astype(BF16)

    def down_away(hf, s):
        q = (y + s) % ny
        down_own(hf, q)
        each(0, hn, lambda t: u_copy(y, q, hf * hn + (me + t) % hn).start())

    def r_copy(src, to):
        return send(fin.at[rows(to, cp)], ret.at[rows(src, cp)], r_s.at[to], r_r.at[src], ep=to)

    def finish(to):
        value = tt[y, rows(to, cp), :].astype(F32)
        for t in range(1, ny):
            q = (y + t) % ny
            u_copy(q, y, to).wait_recv()
            value = value + yr[q, rows(to, cp), :].astype(F32)
        return value.astype(BF16)

    def finish_send(to):
        fin[rows(to, cp), :] = finish(to)
        r_copy(me, to).start()

    each(1, ny + 1, lambda s: down_other(far, (y + s) % ny))
    each(1, ny, lambda s: down_away(far, s))
    down_own(far, y)
    each(1, ny + 1, lambda s: down_other(near, (y + s) % ny))
    each(0, hn, lambda t: finish_send(far * hn + (me + t) % hn))
    each(1, ny, lambda s: down_away(near, s))
    down_own(near, y)
    each(1, hn, lambda t: finish_send(near * hn + (me + t) % hn))
    ret[rows(me, cp), :] = finish(me)

    each(1, ny, lambda s: my_copy((y + s) % ny, y).wait_recv())
    mixed = my[0].astype(F32)
    for j in range(1, ny):
        mixed = mixed + my[j].astype(F32)
    scale = lax.rsqrt(jnp.mean(mixed * mixed, axis=1, keepdims=True) + EPSILON)
    msum_out = (mixed * scale * gain_in[...]).astype(BF16)
    mixer_ref[rows(core, half), :] = msum_out
    mp_copy.wait_send()
    mp[rows(core, half), :] = msum_out
    mo_copy = send(mp.at[rows(core, half)], mo, mo_sem.at[0], mo_sem.at[1], t=mate)
    mo_copy.start()
    mo_copy.wait_recv()
    mixer_ref[rows(other, half), :] = mo[...]

    shared = shs[y].astype(F32) + shr[y].astype(F32)
    for t in range(1, ny):
        q = (y + t) % ny
        v_copy(q, y).wait_recv()
        shared = shared + shv[q].astype(F32)
    each(1, n, lambda s: r_copy((me + n - s) % n, me).wait_recv())
    routed = dot(pick_in[0], ret[...]) + dot(pick_in[1], ret[...])
    expert_ref[...] = (routed + shared).astype(BF16)

    def drain(s):
        to = (me + s) % n
        d_copy(me, to).wait_send()
        r_copy(me, to).wait_send()

        def drain_src(t):
            g_copy(y, (y + t) % ny, to).wait_send()
            u_copy(y, (y + t) % ny, to).wait_send()

        each(1, ny, drain_src)
        each(0, ny, lambda q: m_copy(q, to).wait_send())

    each(1, n, drain)
    each(1, zs, lambda s: kv_copy(me, z_peer(s)).wait_send())
    each(1, xs, lambda s: kv_copy(me, x_peer(s)).wait_send())
    each(1, zs, lambda s: each(1, xs, lambda t: kv_forward((my_z + zs - s) % zs, t).wait_send()))
    own_mate.wait_send()
    sh_copy.wait_send()
    mo_copy.wait_send()
    each(0, ny, lambda q: each(0, 2, lambda hf: p_copy(hf, q).wait_send()))

    def drain_y(s):
        to = (y + s) % ny
        own_y(s).wait_send()
        my_copy(y, to).wait_send()
        v_copy(y, to).wait_send()
        u_copy(y, to, me).wait_send()
        m_copy(to, me).wait_send()

    each(1, ny, drain_y)


def body(
    query_rows, key_rows, value_rows, query_gain, key_gain, out_weight, mixer_gain,
    expert_input, expert_ids, gate_score, expert_gain,
    gate_weight, up_weight, down_weight, shared_gate, shared_up, shared_down,
):
    n = lax.axis_size("ep")
    tp_n = lax.axis_size("tp")
    ny = tp_n // 2
    me = lax.axis_index("ep")
    tp = lax.axis_index("tp")
    ra = query_rows.shape[0]
    heads = query_rows.shape[1] // HEAD_DIM
    first_kv = tp * heads // (HEADS // KV_HEADS)
    angles = rotary_angles(me * ra + jnp.arange(ra, dtype=jnp.int32))
    query_rot = normalize_rotate(query_rows.reshape(ra, heads, HEAD_DIM), query_gain, angles)
    query_rot = query_rot * BF16(HEAD_DIM ** (-0.5))
    q_in = jnp.pad(query_rot.transpose(1, 0, 2), ((0, 0), (0, 0), (0, HEAD_DIM))).reshape(heads * ra, 2 * HEAD_DIM)
    key_cols = lax.dynamic_slice_in_dim(key_rows, first_kv * HEAD_DIM, HEAD_DIM, 1)
    value_cols = lax.dynamic_slice_in_dim(value_rows, first_kv * HEAD_DIM, HEAD_DIM, 1)
    key_rot = normalize_rotate(key_cols.reshape(ra, 1, HEAD_DIM), key_gain, angles)
    kv_in = jnp.concatenate([key_rot.reshape(ra, HEAD_DIM), value_cols], axis=1)
    width = out_weight.shape[1]
    ow_pad = jnp.pad(out_weight.reshape(heads, HEAD_DIM, width), ((0, 0), (HEAD_DIM, 0), (0, 0)))
    ow_pad = ow_pad.reshape(heads * 2 * HEAD_DIM, width)
    rb, top = expert_ids.shape
    experts = n * gate_weight.shape[0]
    cap = 3 * rb * top // (2 * experts)
    cp = -(-cap // 16) * 16
    model = expert_input.shape[1]
    lc = model // tp_n
    widened = expert_input.astype(F32)
    normed = (
        widened * lax.rsqrt(jnp.mean(widened * widened, axis=1, keepdims=True) + EPSILON) * expert_gain
    ).astype(BF16)
    route_weight = gate_score / jnp.sum(gate_score, axis=1, keepdims=True) * ROUTED_SCALE
    named = expert_ids[:, :, None] == jnp.arange(experts, dtype=jnp.int32)
    member = jnp.any(named, axis=1)
    row_weight = jnp.sum(jnp.where(named, route_weight[:, :, None], 0.0), axis=1)
    before = jnp.tril(jnp.ones((rb, rb), BF16), -1)
    rank = dot(before, member.astype(BF16)).astype(jnp.int32)
    slot = jnp.where(member, rank, -1)
    chosen = slot[:, :, None] == jnp.arange(cp, dtype=jnp.int32)
    weight = jnp.where(chosen, row_weight[:, :, None], 0.0).reshape(rb, experts * cp)
    high = weight.astype(BF16)
    low = (weight - high.astype(F32)).astype(BF16)
    pick = jnp.stack([high, low])
    choose = chosen.astype(BF16).reshape(rb, experts * cp)
    own_cols = lax.dynamic_slice_in_dim(normed, tp * lc, lc, 1)
    outgoing = lax.dot_general(
        choose, own_cols, (((0,), (0,)), ((), ())), preferred_element_type=F32
    ).astype(BF16)

    slots = n * cp
    hidden = gate_weight.shape[2]
    sh = shared_gate.shape[1]
    vm = pltpu.VMEM
    dma = pltpu.SemaphoreType.DMA
    half = ra // 2
    vspec = pl.BlockSpec(memory_space=pltpu.VMEM)
    hspec = pl.BlockSpec(memory_space=pl.ANY)
    xs = 1
    while 4 * xs * xs <= n:
        xs *= 2
    sizes = (n, tp_n, ny, heads, cp, lc, xs)
    return pl.pallas_call(
        functools.partial(fused_kernel, sizes),
        out_shape=(
            jax.ShapeDtypeStruct((ra, width), BF16),
            jax.ShapeDtypeStruct((rb, lc), BF16),
        ),
        in_specs=[vspec] * 6 + [hspec] * 7,
        out_specs=(vspec, vspec),
        scratch_shapes=[
            vm((model, sh), BF16), vm((model, sh), BF16), vm((sh, model), BF16),
            vm((heads * 2 * HEAD_DIM, width), BF16),
            vm((model, hidden), BF16), vm((model, hidden), BF16), vm((hidden, model), BF16),
            vm((n * ra, 2 * HEAD_DIM), BF16),
            vm((ra, heads * 2 * HEAD_DIM), BF16),
            vm((ra, width), BF16), vm((half, width), BF16), vm((half, width), BF16),
            vm((ny, half, width), BF16), vm((half, width), BF16),
            vm((tp_n, slots, lc), BF16), vm((slots, hidden), BF16),
            vm((ny, slots, lc), BF16), vm((ny, slots, lc), BF16),
            vm((ny, slots, lc), BF16), vm((ny, slots, lc), BF16),
            vm((slots, lc), BF16), vm((slots, lc), BF16),
            vm((ny, rb, lc), BF16), vm((ny, rb, lc), BF16), vm((ny, rb, lc), BF16),
            vm((ny, rb, lc), BF16), vm((ny, rb, lc), BF16),
            dma((7,)), dma((n,)), dma((n,)), dma((n,)), dma((n,)), dma((n,)),
            dma((ny, n)), dma((ny, n)), dma((ny, n)), dma((ny, n)),
            dma((2,)), dma((ny,)), dma((ny,)), dma((2,)), dma((ny,)), dma((ny,)), dma((2,)),
            dma((2, ny)), dma((2, ny)), dma((ny, n)), dma((ny, n)), dma((n,)), dma((n,)),
        ],
        compiler_params=pltpu.CompilerParams(
            collective_id=0, has_side_effects=True, vmem_limit_bytes=64 * 1024 * 1000
        ),
        name="fused_layer",
    )(
        kv_in, outgoing, q_in, normed, pick, mixer_gain.reshape(1, width),
        shared_gate, shared_up, shared_down, ow_pad,
        gate_weight[0], up_weight[0], down_weight[0],
    )


def solution(mesh):
    in_specs = (
        P("ep", "tp"), P("ep", None), P("ep", None), P(), P(), P("tp", None), P(),
        P("ep", None), P("ep", None), P("ep", None), P(),
        P("ep", None, "tp"), P("ep", None, "tp"), P("ep", "tp", None),
        P(None, "tp"), P(None, "tp"), P("tp", None),
    )
    out_specs = (P("ep", None), P("ep", "tp"))
    return jax.shard_map(body, mesh=mesh, in_specs=in_specs, out_specs=out_specs, check_vma=False)
```

```python
import functools

import jax
import jax.numpy as jnp
import numpy as np
from jax import lax
from jax.experimental import pallas as pl
from jax.experimental.pallas import tpu as pltpu
from jax.sharding import PartitionSpec as P

HEADS = 16
KV_HEADS = 4
HEAD_DIM = 64
GRID_W = 64

EPSILON = 1e-06
ROUTED_SCALE = 2.5
F32 = jnp.float32
BF16 = jnp.bfloat16
MESH = pl.DeviceIdType.MESH


def position_tables(grid_rows):
    quarter = HEAD_DIM // 4
    inverse = (10000.0 ** (-np.arange(quarter, dtype=np.float32) / np.float32(quarter))).astype(np.float32)
    lane = np.arange(2 * HEAD_DIM) % (2 * quarter)
    by_row = lane < quarter
    freq = inverse[lane % quarter]
    sign = np.where(np.arange(2 * HEAD_DIM) % HEAD_DIM < HEAD_DIM // 2, -1.0, 1.0).astype(np.float32)

    def pair(count, used):
        angle = np.arange(count, dtype=np.float32)[:, None] * freq
        return [np.where(used, np.cos(angle), 0.0), np.where(used, np.sin(angle) * sign, 0.0)]

    return np.concatenate(pair(GRID_W, ~by_row) + pair(grid_rows, by_row)).astype(np.float32)


def silu(v):
    return v / (1.0 + jnp.exp(-v))


def dot(a, b):
    return jnp.dot(a, b, preferred_element_type=F32)


def fused_kernel(
    sizes,
    q_ref, k_ref, v_ref, qg_ref, kg_ref, table_ref, gain_ref, x_ref, ids_ref, score_ref, xgain_ref,
    sg_hbm, su_hbm, sd_hbm, ow_hbm, wg_hbm, wu_hbm, wd_hbm,
    mixer_ref, expert_ref,
    sg, su, sd, ow, wg, wu, wd,
    kvo, kv, qs, cosv, sinv, attf, mix, nrm, cht, pick, outf, outn,
    xh, hid, po, rp, tt, yr, fin, ret, sho, shs, shr, shp, shv,
    w_sem, kv_s, kv_r, kf_s, d_s, d_r, m_s, m_r, g_s, g_r, sh_sem, v_s, v_r,
    o_s, o_r, ox_s, ox_r, om_s, om_r, a_s, a_r, am_s, am_r,
    p_s, p_r, u_s, u_r, r_s, r_r,
):
    n, tp_n, ny, heads, cp, lc, xs = sizes
    zs = n // xs
    hn = n // 2
    hs = hn * cp
    me = lax.axis_index("ep")
    tp = lax.axis_index("tp")
    core = tp % 2
    y = tp // 2
    mate = tp + 1 - 2 * core
    other = 1 - core
    my_z = me // xs
    my_x = me % xs
    near = me // hn
    far = 1 - near
    ra = k_ref.shape[0]
    rb, model = x_ref.shape
    slots = n * cp
    hr = ow_hbm.shape[0]
    pr = hr // xs
    pairs = -(-heads // 2)

    def send(src, dst, ssem, rsem, ep=None, t=None):
        return pltpu.make_async_remote_copy(
            src_ref=src, dst_ref=dst, send_sem=ssem, recv_sem=rsem,
            device_id=(me if ep is None else ep, tp if t is None else t), device_id_type=MESH,
        )

    def rows(block, size):
        return pl.ds(pl.multiple_of(block * size, size), size)

    def cols(tile):
        return pl.ds(pl.multiple_of(tile * lc, lc), lc)

    def each(lo, hi, fn):
        def step(i, c):
            fn(i)
            return c
        lax.fori_loop(lo, hi, step, 0)

    weights = [
        pltpu.make_async_copy(a, b, w_sem.at[i])
        for i, (a, b) in enumerate((
            (sg_hbm, sg), (su_hbm, su), (sd_hbm, sd), (ow_hbm, ow.at[rows(tp, hr)]),
            (wg_hbm, wg), (wu_hbm, wu), (wd_hbm, wd)))
    ]
    for copy in weights:
        copy.start()

    barrier = pltpu.get_barrier_semaphore()

    def greet(s):
        pl.semaphore_signal(barrier, inc=1, device_id=((me + s) % n, tp), device_id_type=MESH)

    def greet_y(s):
        pl.semaphore_signal(barrier, inc=1, device_id=(me, (tp + 2 * s) % tp_n), device_id_type=MESH)

    each(1, n, greet)
    each(1, ny, greet_y)
    pl.semaphore_signal(barrier, inc=1, device_id=(me, mate), device_id_type=MESH)

    def kv_copy(src, to):
        return send(kvo, kv.at[rows(src, ra)], kv_s.at[to], kv_r.at[src], ep=to)

    def kv_forward(src_z, s):
        src = src_z * xs + my_x
        x_to = (my_x + s) % xs
        return send(
            kv.at[rows(src, ra)], kv.at[rows(src, ra)], kf_s.at[src_z * xs + x_to], kv_r.at[src], ep=my_z * xs + x_to)

    def z_peer(s):
        return ((my_z + s) % zs) * xs + my_x

    def x_peer(s):
        return my_z * xs + (my_x + s) % xs

    def o_copy(q):
        return send(
            ow_hbm.at[rows(my_x, pr)], ow.at[pl.ds(pl.multiple_of(tp * hr + my_x * pr, pr), pr)],
            o_s.at[q], o_r.at[y], t=2 * q + core)

    def piece(by, x):
        return ow.at[pl.ds(pl.multiple_of((2 * by + core) * hr + x * pr, pr), pr)]

    def o_arrive(by):
        return send(piece(by, my_x), piece(by, my_x), o_s.at[by], o_r.at[by], t=2 * by + core)

    def ox_copy(by, x_to):
        return send(piece(by, my_x), piece(by, my_x), ox_s.at[by, x_to], ox_r.at[by, my_x], ep=my_z * xs + x_to)

    def ox_arrive(by, x_from):
        return send(
            piece(by, x_from), piece(by, x_from), ox_s.at[by, x_from], ox_r.at[by, x_from], ep=my_z * xs + x_from)

    def om_copy(by, side):
        tile = ow.at[rows(2 * by + side, hr)]
        return send(tile, tile, om_s.at[by], om_r.at[by], t=mate)

    pl.semaphore_wait(barrier, n - 1 + ny - 1 + 1)

    each(1, ny, lambda s: o_copy((y + s) % ny).start())

    x = x_ref[...].astype(F32)
    x_scale = lax.rsqrt(jnp.mean(x * x, axis=1, keepdims=True) + EPSILON)
    nrm[...] = (x * x_scale * xgain_ref[...]).astype(BF16)
    elane = lax.broadcasted_iota(jnp.int32, (rb, 128), 1)
    top = ids_ref.shape[1]
    named = [ids_ref[:, k:k + 1] == elane for k in range(top)]
    member = named[0]
    for k in range(1, top):
        member = member | named[k]
    earlier = lax.broadcasted_iota(jnp.int32, (rb, rb), 1) < lax.broadcasted_iota(jnp.int32, (rb, rb), 0)
    rank = dot(jnp.where(earlier, 1.0, 0.0).astype(BF16), jnp.where(member, 1.0, 0.0).astype(BF16))
    slot = jnp.where(member, rank, -1.0)
    slot_t = slot.T
    place = lax.broadcasted_iota(jnp.int32, (cp, rb), 0).astype(F32)
    for e in range(n):
        cht[e * cp:(e + 1) * cp, :] = jnp.where(slot_t[e:e + 1, :] == place, 1.0, 0.0).astype(BF16)

    def d_near(q, src, to):
        return send(
            outn.at[q, rows(to % hn, cp)], xh.at[2 * q + core, rows(src, cp)], d_s.at[q, to], d_r.at[q, src], ep=to)

    def d_far(src, to):
        return send(outf.at[rows(to % hn, cp)], xh.at[tp, rows(src, cp)], d_s.at[y, to], d_r.at[y, src], ep=to)

    def near_peer(s):
        return near * hn + (me + s) % hn

    def far_peer(s):
        return far * hn + (me + s) % hn

    for q in range(ny):
        outn[q] = dot(cht[rows(near, hs), :], nrm[:, cols(2 * q + core)]).astype(BF16)
        each(1, hn, lambda s: d_near(q, me, near_peer(s)).start())
    outf[...] = dot(cht[rows(far, hs), :], nrm[:, cols(tp)]).astype(BF16)
    each(0, hn, lambda s: d_far(me, far_peer(s)).start())
    for j in range(tp_n):
        xh[j, rows(me, cp), :] = dot(cht[rows(me, cp), :], nrm[:, j * lc:(j + 1) * lc]).astype(BF16)

    with jax.named_scope("shared"):
        for i in range(3):
            weights[i].wait()
        normed = nrm[...]
        sh_hidden = (silu(dot(normed, sg[...])) * dot(normed, su[...])).astype(BF16)
        for q in range(ny):
            sho[q] = dot(sh_hidden, sd[:, cols(2 * q + other)]).astype(BF16)
        sh_copy = send(sho, shr, sh_sem.at[0], sh_sem.at[1], t=mate)
        sh_copy.start()
        for q in range(ny):
            shs[q] = dot(sh_hidden, sd[:, cols(2 * q + core)]).astype(BF16)

    def v_copy(by, q):
        return send(shp.at[q], shv.at[by], v_s.at[q], v_r.at[by], t=2 * q + core)

    lane = lax.broadcasted_iota(jnp.int32, (1, 2 * HEAD_DIM), 1)
    left = lane < HEAD_DIM
    front = lane % HEAD_DIM < HEAD_DIM // 2
    grid_rows = (table_ref.shape[0] - 2 * GRID_W) // 2
    for g in range(ra // GRID_W):
        at = slice(g * GRID_W, (g + 1) * GRID_W)
        line = 2 * GRID_W + me * (ra // GRID_W) + g
        cosv[at, :] = table_ref[0:GRID_W, :] + table_ref[pl.ds(line, 1), :]
        sinv[at, :] = table_ref[GRID_W:2 * GRID_W, :] + table_ref[pl.ds(line + grid_rows, 1), :]

    def rotate(v):
        swapped = jnp.where(front, pltpu.roll(v, 3 * HEAD_DIM // 2, 1), pltpu.roll(v, HEAD_DIM // 2, 1))
        return v * cosv[...] + swapped * sinv[...]

    def inverse_rms(total):
        return lax.rsqrt(total * (1.0 / HEAD_DIM) + EPSILON)

    first_kv = tp * heads // (HEADS // KV_HEADS)
    kv_at = rows(first_kv // 2, 2 * HEAD_DIM)
    odd = (jnp.zeros((1, 2 * HEAD_DIM), jnp.int32) + first_kv % 2) == 1
    k_two = k_ref[:, kv_at].astype(F32)
    v_two = v_ref[:, kv_at].astype(F32)
    k_own = jnp.where(odd, pltpu.roll(k_two, HEAD_DIM, 1), k_two)
    v_own = jnp.where(odd, v_two, pltpu.roll(v_two, HEAD_DIM, 1))
    k_sum = jnp.sum(jnp.where(left, k_own * k_own, 0.0), axis=1, keepdims=True)
    k_turned = rotate(k_own * inverse_rms(k_sum) * kg_ref[...])
    kv_mine = jnp.where(left, k_turned, v_own).astype(BF16)
    kvo[...] = kv_mine
    kv[rows(me, ra), :] = kv_mine

    with jax.named_scope("queries"):
        for p in range(pairs):
            q_two = q_ref[:, p * 128:(p + 1) * 128].astype(F32)
            square = q_two * q_two
            low = inverse_rms(jnp.sum(jnp.where(left, square, 0.0), axis=1, keepdims=True))
            high = inverse_rms(jnp.sum(jnp.where(left, 0.0, square), axis=1, keepdims=True))
            turned = rotate(q_two * jnp.where(left, low, high) * qg_ref[...]) * HEAD_DIM ** (-0.5)
            qs[2 * p * ra:(2 * p + 1) * ra, :] = jnp.where(left, turned, 0.0).astype(BF16)
            if 2 * p + 1 < heads:
                qs[(2 * p + 1) * ra:(2 * p + 2) * ra, :] = jnp.where(
                    left, pltpu.roll(turned, HEAD_DIM, 1), 0.0).astype(BF16)

    with jax.named_scope("shared_pair"):
        sh_copy.wait_recv()
        for q in range(ny):
            shp[q] = (shs[q].astype(F32) + shr[q].astype(F32)).astype(BF16)
    weights[3].wait()
    om_copy(y, core).start()

    def kv_pass(s):
        src_z = (my_z + zs - s) % zs
        kv_copy(src_z * xs + my_x, me).wait_recv()
        each(1, xs, lambda t: kv_forward(src_z, t).start())

    with jax.named_scope("pick"):
        total_score = score_ref[:, 0:1]
        for k in range(1, top):
            total_score = total_score + score_ref[:, k:k + 1]
        row_weight = jnp.zeros((rb, 128), F32)
        for k in range(top):
            row_weight = row_weight + jnp.where(named[k], score_ref[:, k:k + 1] / total_score * ROUTED_SCALE, 0.0)
        high_w = row_weight.astype(BF16)
        low_w = (row_weight - high_w.astype(F32)).astype(BF16)
        slot_lane = lax.broadcasted_iota(jnp.int32, (1, slots), 1).astype(F32)
        slot_expert = jnp.floor((slot_lane + 0.5) * (1.0 / cp))
        spread = jnp.where(
            lax.broadcasted_iota(jnp.int32, (128, slots), 0).astype(F32) == slot_expert, 1.0, 0.0).astype(BF16)
        chosen = dot(slot.astype(BF16), spread) == slot_lane - slot_expert * cp
        pick[0] = jnp.where(chosen, dot(high_w, spread), 0.0).astype(BF16)
        pick[1] = jnp.where(chosen, dot(low_w, spread), 0.0).astype(BF16)

    def kv_rest(s):
        x_from = (my_x + xs - s) % xs
        each(0, zs, lambda t: kv_copy(((my_z + t) % zs) * xs + x_from, me).wait_recv())

    def m_copy(q, src):
        block = xh.at[2 * q + core, rows(src, cp)]
        return send(block, block, m_s.at[q, src], m_r.at[q, src], t=mate)

    def m_arrive(q, src):
        block = xh.at[2 * q + other, rows(src, cp)]
        return send(block, block, m_s.at[q, src], m_r.at[q, src], t=mate)

    def g_copy(by, q, src):
        block = xh.at[2 * by + core, rows(src, cp)]
        return send(block, block, g_s.at[q, src], g_r.at[by, src], t=2 * q + core)

    def near_src(s):
        return near * hn + (me + hn - s) % hn

    def far_src(s):
        return far * hn + (me + hn - s) % hn

    def near_pass(s):
        src = near_src(s)

        def one(q):
            d_near(q, src, me).wait_recv()
            m_copy(q, src).start()

        each(0, ny, one)

    def far_pass(s):
        src = far_src(s)
        d_far(src, me).wait_recv()
        each(1, ny, lambda t: g_copy(y, (y + t) % ny, src).start())
        m_copy(y, src).start()

    def far_pass_y(s):
        src = far_src(s)

        def one(t):
            q = (y + t) % ny
            g_copy(q, y, src).wait_recv()
            m_copy(q, src).start()

        each(1, ny, one)

    def ow_pass():
        def one(s):
            by = (y + s) % ny
            o_arrive(by).wait_recv()
            each(1, xs, lambda t: ox_copy(by, (my_x + t) % xs).start())

        each(1, ny, one)

    def ow_last():
        def one(s):
            by = (y + s) % ny
            each(1, xs, lambda t: ox_arrive(by, (my_x + t) % xs).wait_recv())
            om_copy(by, core).start()

        each(1, ny, one)

    total = kv.shape[0]
    bq = max(16, min(ra, 128 * 3072 // total // 16 * 16))
    while ra % bq:
        bq -= 16
    per_head = ra // bq

    def attend(head, i):
        block = qs[rows(head * per_head + i, bq), :]
        scores = lax.dot_general(block, kv[...], (((1,), (1,)), ((), ())), preferred_element_type=F32)
        peak = jnp.max(scores, axis=1, keepdims=True)
        exponent = jnp.exp(scores - peak)
        row_total = jnp.sum(exponent, axis=1, keepdims=True)
        return dot(exponent.astype(BF16), kv[...]) / row_total

    turns = pairs * per_head

    def attend_turn(i):
        p = i // per_head
        b = i % per_head
        first = attend(2 * p, b)
        if heads > 1:
            both = jnp.where(left, pltpu.roll(first, HEAD_DIM, 1), attend(2 * p + 1, b))
            attf[tp, rows(b, bq), rows(p, 128)] = both.astype(BF16)
        else:
            attf[tp, rows(b, bq), :] = first[:, HEAD_DIM:].astype(BF16)
        each(i * hn // turns, (i + 1) * hn // turns, lambda s: finish_send(far_peer(s)))

    def far_step(s):
        far_pass(s)
        each(jnp.maximum(s - 1, 0), s, far_pass_y)

    def a_copy(by, q):
        return send(attf.at[2 * by + core], attf.at[2 * by + core], a_s.at[q], a_r.at[by], t=2 * q + core)

    def am_copy(by, side):
        return send(attf.at[2 * by + side], attf.at[2 * by + side], am_s.at[by], am_r.at[by], t=mate)

    ft = min(256, hid.shape[1])

    def gate_up(hf, t):
        at = pl.ds(pl.multiple_of(t * ft, ft), ft)
        gate = dot(xh[0, rows(hf, hs), :], wg[0:lc, at])
        up = dot(xh[0, rows(hf, hs), :], wu[0:lc, at])
        for j in range(1, tp_n):
            gate = gate + dot(xh[j, rows(hf, hs), :], wg[j * lc:(j + 1) * lc, at])
            up = up + dot(xh[j, rows(hf, hs), :], wu[j * lc:(j + 1) * lc, at])
        hid[rows(hf, hs), at] = (silu(gate) * up).astype(BF16)

    def p_copy(hf, q):
        return send(po.at[q, rows(hf, hs)], rp.at[q, rows(hf, hs)], p_s.at[hf, q], p_r.at[hf, q], t=mate)

    def down_other(hf, q):
        po[q, rows(hf, hs), :] = dot(hid[rows(hf, hs), :], wd[:, cols(2 * q + other)]).astype(BF16)
        p_copy(hf, q).start()

    def u_copy(by, q, to):
        return send(tt.at[q, rows(to, cp)], yr.at[by, rows(to, cp)], u_s.at[q, to], u_r.at[by, to], t=2 * q + core)

    def down_own(hf, q):
        own = dot(hid[rows(hf, hs), :], wd[:, cols(2 * q + core)]).astype(BF16).astype(F32)
        p_copy(hf, q).wait_recv()
        tt[q, rows(hf, hs), :] = (own + rp[q, rows(hf, hs), :].astype(F32)).astype(BF16)

    def down_away(hf, s):
        q = (y + s) % ny
        down_own(hf, q)
        each(0, hn, lambda t: u_copy(y, q, hf * hn + (me + t) % hn).start())

    def r_copy(src, to):
        return send(fin.at[rows(to, cp)], ret.at[rows(src, cp)], r_s.at[to], r_r.at[src], ep=to)

    def finish(to):
        value = tt[y, rows(to, cp), :].astype(F32)
        for t in range(1, ny):
            q = (y + t) % ny
            u_copy(q, y, to).wait_recv()
            value = value + yr[q, rows(to, cp), :].astype(F32)
        return value.astype(BF16)

    def finish_send(to):
        fin[rows(to, cp), :] = finish(to)
        r_copy(me, to).start()

    def near_wait(s):
        each(0, ny, lambda q: m_arrive(q, near_src(s)).wait_recv())

    def far_wait(s):
        each(0, ny, lambda q: m_arrive(q, far_src(s)).wait_recv())

    tiles = hid.shape[1] // ft

    def near_tile(t):
        gate_up(near, t)
        each(t * hn // tiles, (t + 1) * hn // tiles, far_step)

    def far_tile(t):
        gate_up(far, t)
        each(1 + t * (zs - 1) // tiles, 1 + (t + 1) * (zs - 1) // tiles, kv_pass)

    with jax.named_scope("near_pass"):
        each(1, hn, near_pass)
    with jax.named_scope("near_wait"):
        weights[4].wait()
        weights[5].wait()
        each(1, hn, near_wait)
    each(1, zs, lambda s: kv_copy(me, z_peer(s)).start())
    each(1, xs, lambda s: kv_copy(me, x_peer(s)).start())
    with jax.named_scope("near_gate_up"):
        each(0, tiles, near_tile)
    with jax.named_scope("near_down"):
        weights[6].wait()
        each(1, ny + 1, lambda s: down_other(near, (y + s) % ny))
        far_pass_y(hn - 1)
        each(1, ny, lambda s: down_away(near, s))
        down_own(near, y)
    with jax.named_scope("far_wait"):
        each(0, hn, far_wait)
    with jax.named_scope("far_gate_up"):
        each(0, tiles, far_tile)
    with jax.named_scope("ow_pass"):
        ow_pass()
    with jax.named_scope("far_down"):
        each(1, ny + 1, lambda s: down_other(far, (y + s) % ny))
        each(1, ny, lambda s: down_away(far, s))
        down_own(far, y)
    each(1, ny, lambda s: v_copy(y, (y + s) % ny).start())
    with jax.named_scope("finish_near"):
        each(1, hn, lambda s: finish_send(near_peer(s)))
        ret[rows(me, cp), :] = finish(me)
    with jax.named_scope("kv_rest"):
        each(1, xs, kv_rest)
    with jax.named_scope("attend"):
        each(0, turns, attend_turn)
    am_copy(y, core).start()
    each(1, ny, lambda s: a_copy(y, (y + s) % ny).start())

    with jax.named_scope("ow_last"):
        ow_last()
    with jax.named_scope("att_wait"):
        def att_pass(s):
            by = (y + s) % ny
            a_copy(by, y).wait_recv()
            am_copy(by, core).start()

        each(1, ny, att_pass)
    with jax.named_scope("mixer"):
        each(0, ny, lambda by: am_copy(by, other).wait_recv())
        each(0, ny, lambda by: om_copy(by, other).wait_recv())
        width = mix.shape[1]
        tile = min(512, width)

        def project(t, ssq):
            at = pl.ds(pl.multiple_of(t * tile, tile), tile)
            part = dot(attf[0], ow[0:hr, at])
            for j in range(1, tp_n):
                part = part + dot(attf[j], ow[j * hr:(j + 1) * hr, at])
            mix[:, at] = part
            return ssq + jnp.sum(part * part, axis=1, keepdims=True)

        ssq = lax.fori_loop(0, width // tile, project, jnp.zeros((ra, 1), F32))
        scale = lax.rsqrt(ssq * (1.0 / width) + EPSILON)
        mixer_ref[...] = (mix[...] * scale * gain_ref[...]).astype(BF16)

    shared = shs[y].astype(F32) + shr[y].astype(F32)
    for t in range(1, ny):
        q = (y + t) % ny
        v_copy(q, y).wait_recv()
        shared = shared + shv[q].astype(F32)
    with jax.named_scope("ret_wait"):
        each(1, n, lambda s: r_copy((me + n - s) % n, me).wait_recv())
    expert_ref[...] = (dot(pick[0], ret[...]) + dot(pick[1], ret[...]) + shared).astype(BF16)

    def drain(s):
        to = (me + s) % n
        r_copy(me, to).wait_send()
        each(0, ny, lambda q: m_copy(q, to).wait_send())
        each(1, ny, lambda t: u_copy(y, (y + t) % ny, to).wait_send())

    def drain_far(s):
        d_far(me, far_peer(s)).wait_send()
        each(1, ny, lambda t: g_copy(y, (y + t) % ny, far_peer(s)).wait_send())

    def drain_y(s):
        q = (y + s) % ny
        o_copy(q).wait_send()
        each(1, xs, lambda t: ox_copy(q, (my_x + t) % xs).wait_send())
        a_copy(y, q).wait_send()
        v_copy(y, q).wait_send()
        u_copy(y, q, me).wait_send()

    with jax.named_scope("drain"):
        each(1, n, drain)
        each(0, hn, drain_far)
        each(1, hn, lambda s: each(0, ny, lambda q: d_near(q, me, near_peer(s)).wait_send()))
        each(1, zs, lambda s: kv_copy(me, z_peer(s)).wait_send())
        each(1, xs, lambda s: kv_copy(me, x_peer(s)).wait_send())
        each(1, zs, lambda s: each(1, xs, lambda t: kv_forward((my_z + zs - s) % zs, t).wait_send()))
        sh_copy.wait_send()
        each(0, ny, lambda q: each(0, 2, lambda hf: p_copy(hf, q).wait_send()))
        each(0, ny, lambda by: om_copy(by, core).wait_send())
        each(0, ny, lambda by: am_copy(by, core).wait_send())
        each(1, ny, drain_y)


def body(
    query_rows, key_rows, value_rows, query_gain, key_gain, out_weight, mixer_gain,
    expert_input, expert_ids, gate_score, expert_gain,
    gate_weight, up_weight, down_weight, shared_gate, shared_up, shared_down,
):
    n = lax.axis_size("ep")
    tp_n = lax.axis_size("tp")
    ny = tp_n // 2
    ra = query_rows.shape[0]
    heads = query_rows.shape[1] // HEAD_DIM
    width = out_weight.shape[1]
    rb, top = expert_ids.shape
    experts = n * gate_weight.shape[0]
    cap = 3 * rb * top // (2 * experts)
    cp = -(-cap // 16) * 16
    model = expert_input.shape[1]
    lc = model // tp_n
    xs = 1
    while 4 * xs * xs <= n:
        xs *= 2
    if heads % 2:
        query_rows = jnp.pad(query_rows, ((0, 0), (0, HEAD_DIM)))
    pairs = -(-heads // 2)
    table = jnp.asarray(position_tables(n * ra // GRID_W))
    q_gain = jnp.concatenate([query_gain, query_gain]).reshape(1, 2 * HEAD_DIM)
    k_gain = jnp.concatenate([key_gain, key_gain]).reshape(1, 2 * HEAD_DIM)

    slots = n * cp
    hidden = gate_weight.shape[2]
    sh = shared_gate.shape[1]
    hr = heads * HEAD_DIM
    vm = pltpu.VMEM
    dma = pltpu.SemaphoreType.DMA
    vspec = pl.BlockSpec(memory_space=pltpu.VMEM)
    hspec = pl.BlockSpec(memory_space=pl.ANY)
    sizes = (n, tp_n, ny, heads, cp, lc, xs)
    return pl.pallas_call(
        functools.partial(fused_kernel, sizes),
        out_shape=(
            jax.ShapeDtypeStruct((ra, width), BF16),
            jax.ShapeDtypeStruct((rb, lc), BF16),
        ),
        in_specs=[vspec] * 11 + [hspec] * 7,
        out_specs=(vspec, vspec),
        scratch_shapes=[
            vm((model, sh), BF16), vm((model, sh), BF16), vm((sh, model), BF16),
            vm((tp_n * hr, width), BF16),
            vm((model, hidden), BF16), vm((model, hidden), BF16), vm((hidden, model), BF16),
            vm((ra, 2 * HEAD_DIM), BF16), vm((n * ra, 2 * HEAD_DIM), BF16), vm((2 * pairs * ra, 2 * HEAD_DIM), BF16),
            vm((ra, 2 * HEAD_DIM), F32), vm((ra, 2 * HEAD_DIM), F32),
            vm((tp_n, ra, hr), BF16), vm((ra, width), F32),
            vm((rb, model), BF16), vm((slots, rb), BF16), vm((2, rb, slots), BF16),
            vm((slots // 2, lc), BF16), vm((ny, slots // 2, lc), BF16),
            vm((tp_n, slots, lc), BF16), vm((slots, hidden), BF16),
            vm((ny, slots, lc), BF16), vm((ny, slots, lc), BF16),
            vm((ny, slots, lc), BF16), vm((ny, slots, lc), BF16),
            vm((slots, lc), BF16), vm((slots, lc), BF16),
            vm((ny, rb, lc), BF16), vm((ny, rb, lc), BF16), vm((ny, rb, lc), BF16),
            vm((ny, rb, lc), BF16), vm((ny, rb, lc), BF16),
            dma((7,)), dma((n,)), dma((n,)), dma((n,)), dma((ny, n)), dma((ny, n)),
            dma((ny, n)), dma((ny, n)), dma((ny, n)), dma((ny, n)), dma((2,)), dma((ny,)), dma((ny,)),
            dma((ny,)), dma((ny,)), dma((ny, xs)), dma((ny, xs)), dma((ny,)), dma((ny,)),
            dma((ny,)), dma((ny,)), dma((ny,)), dma((ny,)),
            dma((2, ny)), dma((2, ny)), dma((ny, n)), dma((ny, n)), dma((n,)), dma((n,)),
        ],
        compiler_params=pltpu.CompilerParams(
            collective_id=0, has_side_effects=True, vmem_limit_bytes=64 * 1024 * 1000
        ),
        name="fused_layer",
    )(
        query_rows, key_rows, value_rows, q_gain, k_gain, table, mixer_gain.reshape(1, width),
        expert_input, expert_ids, gate_score, expert_gain.reshape(1, model),
        shared_gate, shared_up, shared_down, out_weight,
        gate_weight[0], up_weight[0], down_weight[0],
    )


def solution(mesh):
    in_specs = (
        P("ep", "tp"), P("ep", None), P("ep", None), P(), P(), P("tp", None), P(),
        P("ep", None), P("ep", None), P("ep", None), P(),
        P("ep", None, "tp"), P("ep", None, "tp"), P("ep", "tp", None),
        P(None, "tp"), P(None, "tp"), P("tp", None),
    )
    out_specs = (P("ep", None), P("ep", "tp"))
    return jax.shard_map(body, mesh=mesh, in_specs=in_specs, out_specs=out_specs, check_vma=False)
```

```python
import functools

import jax
import jax.numpy as jnp
import numpy as np
from jax import lax
from jax.experimental import pallas as pl
from jax.experimental.pallas import tpu as pltpu
from jax.sharding import PartitionSpec as P

HEADS = 16
KV_HEADS = 4
HEAD_DIM = 64
GRID_W = 64

EPSILON = 1e-06
ROUTED_SCALE = 2.5
F32 = jnp.float32
BF16 = jnp.bfloat16
MESH = pl.DeviceIdType.MESH


def position_tables(grid_rows):
    quarter = HEAD_DIM // 4
    inverse = (10000.0 ** (-np.arange(quarter, dtype=np.float32) / np.float32(quarter))).astype(np.float32)
    lane = np.arange(2 * HEAD_DIM) % (2 * quarter)
    by_row = lane < quarter
    freq = inverse[lane % quarter]
    sign = np.where(np.arange(2 * HEAD_DIM) % HEAD_DIM < HEAD_DIM // 2, -1.0, 1.0).astype(np.float32)

    def pair(count, used):
        angle = np.arange(count, dtype=np.float32)[:, None] * freq
        return [np.where(used, np.cos(angle), 0.0), np.where(used, np.sin(angle) * sign, 0.0)]

    return np.concatenate(pair(GRID_W, ~by_row) + pair(grid_rows, by_row)).astype(np.float32)


def query_block(ra, total):
    bq = max(16, min(ra, 128 * 3072 // total // 16 * 16))
    while ra % bq:
        bq -= 16
    return bq


def silu(v):
    return v / (1.0 + jnp.exp(-v))


def dot(a, b):
    return jnp.dot(a, b, preferred_element_type=F32)


def fused_kernel(
    sizes,
    q_ref, k_ref, v_ref, qg_ref, kg_ref, table_ref, gain_ref, x_ref, ids_ref, score_ref, xgain_ref,
    sg_hbm, su_hbm, sd_hbm, ow_hbm, wg_hbm, wu_hbm, wd_hbm,
    mixer_ref, expert_ref,
    sg, su, sd, ow, wg, wu, wd,
    kvo, kv, qs, cosv, sinv, attf, mix, nrm, cht, pick, outf, outn,
    xh, hid, po, rp, tt, yr, fin, ret, sho, shs, shr, shp, shv,
    w_sem, kv_s, kv_r, kf_s, d_s, d_r, m_s, m_r, g_s, g_r, sh_sem, v_s, v_r,
    o_s, o_r, ox_s, ox_r, om_s, om_r, a_s, a_r, am_s, am_r,
    p_s, p_r, u_s, u_r, r_s, r_r,
):
    n, tp_n, ny, heads, cp, lc, xs = sizes
    zs = n // xs
    hn = n // 2
    hs = hn * cp
    me = lax.axis_index("ep")
    tp = lax.axis_index("tp")
    core = tp % 2
    y = tp // 2
    mate = tp + 1 - 2 * core
    other = 1 - core
    my_z = me // xs
    my_x = me % xs
    near = me // hn
    far = 1 - near
    ra = k_ref.shape[0]
    rb, model = x_ref.shape
    slots = n * cp
    hr = ow_hbm.shape[0]
    pr = hr // xs
    pairs = -(-heads // 2)

    def send(src, dst, ssem, rsem, ep=None, t=None):
        return pltpu.make_async_remote_copy(
            src_ref=src, dst_ref=dst, send_sem=ssem, recv_sem=rsem,
            device_id=(me if ep is None else ep, tp if t is None else t), device_id_type=MESH,
        )

    def rows(block, size):
        return pl.ds(pl.multiple_of(block * size, size), size)

    def cols(tile):
        return pl.ds(pl.multiple_of(tile * lc, lc), lc)

    def each(lo, hi, fn):
        def step(i, c):
            fn(i)
            return c
        lax.fori_loop(lo, hi, step, 0)

    weights = [
        pltpu.make_async_copy(a, b, w_sem.at[i])
        for i, (a, b) in enumerate((
            (sg_hbm, sg), (su_hbm, su), (sd_hbm, sd), (ow_hbm, ow.at[rows(tp, hr)]),
            (wg_hbm, wg), (wu_hbm, wu), (wd_hbm, wd)))
    ]
    for copy in weights:
        copy.start()

    barrier = pltpu.get_barrier_semaphore()

    def greet(s):
        pl.semaphore_signal(barrier, inc=1, device_id=((me + s) % n, tp), device_id_type=MESH)

    def greet_y(s):
        pl.semaphore_signal(barrier, inc=1, device_id=(me, (tp + 2 * s) % tp_n), device_id_type=MESH)

    each(1, n, greet)
    each(1, ny, greet_y)
    pl.semaphore_signal(barrier, inc=1, device_id=(me, mate), device_id_type=MESH)

    def kv_copy(src, to):
        return send(kvo, kv.at[rows(src, ra)], kv_s.at[to], kv_r.at[src], ep=to)

    def kv_forward(src_z, s):
        src = src_z * xs + my_x
        x_to = (my_x + s) % xs
        return send(
            kv.at[rows(src, ra)], kv.at[rows(src, ra)], kf_s.at[src_z * xs + x_to], kv_r.at[src], ep=my_z * xs + x_to)

    def z_peer(s):
        return ((my_z + s) % zs) * xs + my_x

    def x_peer(s):
        return my_z * xs + (my_x + s) % xs

    def o_copy(q):
        return send(
            ow_hbm.at[rows(my_x, pr)], ow.at[pl.ds(pl.multiple_of(tp * hr + my_x * pr, pr), pr)],
            o_s.at[q], o_r.at[y], t=2 * q + core)

    def piece(by, x):
        return ow.at[pl.ds(pl.multiple_of((2 * by + core) * hr + x * pr, pr), pr)]

    def o_arrive(by):
        return send(piece(by, my_x), piece(by, my_x), o_s.at[by], o_r.at[by], t=2 * by + core)

    def ox_copy(by, x_to):
        return send(piece(by, my_x), piece(by, my_x), ox_s.at[by, x_to], ox_r.at[by, my_x], ep=my_z * xs + x_to)

    def ox_arrive(by, x_from):
        return send(
            piece(by, x_from), piece(by, x_from), ox_s.at[by, x_from], ox_r.at[by, x_from], ep=my_z * xs + x_from)

    def om_copy(by, side):
        tile = ow.at[rows(2 * by + side, hr)]
        return send(tile, tile, om_s.at[by], om_r.at[by], t=mate)

    with jax.named_scope("barrier"):
        pl.semaphore_wait(barrier, n - 1 + ny - 1 + 1)

    each(1, ny, lambda s: o_copy((y + s) % ny).start())

    x = x_ref[...].astype(F32)
    x_scale = lax.rsqrt(jnp.mean(x * x, axis=1, keepdims=True) + EPSILON)
    nrm[...] = (x * x_scale * xgain_ref[...]).astype(BF16)
    erow = lax.broadcasted_iota(jnp.int32, (128, rb), 0)
    top = ids_ref.shape[0]
    named = [ids_ref[k:k + 1, :] == erow for k in range(top)]
    member = named[0]
    for k in range(1, top):
        member = member | named[k]
    earlier = lax.broadcasted_iota(jnp.int32, (rb, rb), 0) < lax.broadcasted_iota(jnp.int32, (rb, rb), 1)
    rank = dot(jnp.where(member, 1.0, 0.0).astype(BF16), jnp.where(earlier, 1.0, 0.0).astype(BF16))
    slot_t = jnp.where(member, rank, -1.0)
    place = lax.broadcasted_iota(jnp.int32, (cp, rb), 0).astype(F32)
    for e in range(n):
        cht[e * cp:(e + 1) * cp, :] = jnp.where(slot_t[e:e + 1, :] == place, 1.0, 0.0).astype(BF16)

    def d_near(q, src, to):
        return send(
            outn.at[q, rows(to % hn, cp)], xh.at[2 * q + core, rows(src, cp)], d_s.at[q, to], d_r.at[q, src], ep=to)

    def d_far(src, to):
        return send(outf.at[rows(to % hn, cp)], xh.at[tp, rows(src, cp)], d_s.at[y, to], d_r.at[y, src], ep=to)

    def near_peer(s):
        return near * hn + (me + s) % hn

    def far_peer(s):
        return far * hn + (me + s) % hn

    for q in range(ny):
        outn[q] = dot(cht[rows(near, hs), :], nrm[:, cols(2 * q + core)]).astype(BF16)
        each(1, hn, lambda s: d_near(q, me, near_peer(s)).start())
    outf[...] = dot(cht[rows(far, hs), :], nrm[:, cols(tp)]).astype(BF16)
    each(0, hn, lambda s: d_far(me, far_peer(s)).start())
    for j in range(tp_n):
        xh[j, rows(me, cp), :] = dot(cht[rows(me, cp), :], nrm[:, j * lc:(j + 1) * lc]).astype(BF16)

    with jax.named_scope("shared"):
        for i in range(3):
            weights[i].wait()
        normed = nrm[...]
        sh_hidden = (silu(dot(normed, sg[...])) * dot(normed, su[...])).astype(BF16)
        for q in range(ny):
            sho[q] = dot(sh_hidden, sd[:, cols(2 * q + other)]).astype(BF16)
        sh_copy = send(sho, shr, sh_sem.at[0], sh_sem.at[1], t=mate)
        sh_copy.start()
        for q in range(ny):
            shs[q] = dot(sh_hidden, sd[:, cols(2 * q + core)]).astype(BF16)

    def v_copy(by, q):
        return send(shp.at[q], shv.at[by], v_s.at[q], v_r.at[by], t=2 * q + core)

    lane = lax.broadcasted_iota(jnp.int32, (1, 2 * HEAD_DIM), 1)
    left = lane < HEAD_DIM
    front = lane % HEAD_DIM < HEAD_DIM // 2
    grid_rows = (table_ref.shape[0] - 2 * GRID_W) // 2
    for g in range(ra // GRID_W):
        at = slice(g * GRID_W, (g + 1) * GRID_W)
        line = 2 * GRID_W + me * (ra // GRID_W) + g
        cosv[at, :] = table_ref[0:GRID_W, :] + table_ref[pl.ds(line, 1), :]
        sinv[at, :] = table_ref[GRID_W:2 * GRID_W, :] + table_ref[pl.ds(line + grid_rows, 1), :]

    def rotate(v):
        swapped = jnp.where(front, pltpu.roll(v, 3 * HEAD_DIM // 2, 1), pltpu.roll(v, HEAD_DIM // 2, 1))
        return v * cosv[...] + swapped * sinv[...]

    def inverse_rms(total):
        return lax.rsqrt(total * (1.0 / HEAD_DIM) + EPSILON)

    first_kv = tp * heads // (HEADS // KV_HEADS)
    kv_at = rows(first_kv // 2, 2 * HEAD_DIM)
    odd = (jnp.zeros((1, 2 * HEAD_DIM), jnp.int32) + first_kv % 2) == 1
    k_two = k_ref[:, kv_at].astype(F32)
    v_two = v_ref[:, kv_at].astype(F32)
    k_own = jnp.where(odd, pltpu.roll(k_two, HEAD_DIM, 1), k_two)
    v_own = jnp.where(odd, v_two, pltpu.roll(v_two, HEAD_DIM, 1))
    k_sum = jnp.sum(jnp.where(left, k_own * k_own, 0.0), axis=1, keepdims=True)
    k_turned = rotate(k_own * inverse_rms(k_sum) * jnp.concatenate([kg_ref[...]] * 2, axis=1))
    kv_mine = jnp.where(left, k_turned, v_own).astype(BF16)
    kvo[...] = kv_mine
    kv[rows(me, ra), :] = kv_mine

    with jax.named_scope("queries"):
        q_gain = jnp.concatenate([qg_ref[...]] * 2, axis=1)
        for p in range(pairs):
            q_two = q_ref[:, p * 128:(p + 1) * 128].astype(F32)
            square = q_two * q_two
            low = inverse_rms(jnp.sum(jnp.where(left, square, 0.0), axis=1, keepdims=True))
            high = inverse_rms(jnp.sum(jnp.where(left, 0.0, square), axis=1, keepdims=True))
            turned = rotate(q_two * jnp.where(left, low, high) * q_gain) * HEAD_DIM ** (-0.5)
            qs[2 * p * ra:(2 * p + 1) * ra, :] = jnp.where(left, turned, 0.0).astype(BF16)
            if 2 * p + 1 < heads:
                qs[(2 * p + 1) * ra:(2 * p + 2) * ra, :] = jnp.where(
                    left, pltpu.roll(turned, HEAD_DIM, 1), 0.0).astype(BF16)

    with jax.named_scope("shared_pair"):
        sh_copy.wait_recv()
        for q in range(ny):
            shp[q] = (shs[q].astype(F32) + shr[q].astype(F32)).astype(BF16)
    weights[3].wait()
    om_copy(y, core).start()

    def kv_pass(s):
        src_z = (my_z + zs - s) % zs
        kv_copy(src_z * xs + my_x, me).wait_recv()
        each(1, xs, lambda t: kv_forward(src_z, t).start())

    with jax.named_scope("pick"):
        total_score = score_ref[0:1, :]
        for k in range(1, top):
            total_score = total_score + score_ref[k:k + 1, :]
        weight_t = jnp.zeros((128, rb), F32)
        for k in range(top):
            weight_t = weight_t + jnp.where(named[k], score_ref[k:k + 1, :] / total_score * ROUTED_SCALE, 0.0)
        row_weight = weight_t.T
        slot = slot_t.T
        high_w = row_weight.astype(BF16)
        low_w = (row_weight - high_w.astype(F32)).astype(BF16)
        slot_lane = lax.broadcasted_iota(jnp.int32, (1, slots), 1).astype(F32)
        slot_expert = jnp.floor((slot_lane + 0.5) * (1.0 / cp))
        spread = jnp.where(
            lax.broadcasted_iota(jnp.int32, (128, slots), 0).astype(F32) == slot_expert, 1.0, 0.0).astype(BF16)
        chosen = dot(slot.astype(BF16), spread) == slot_lane - slot_expert * cp
        pick[0] = jnp.where(chosen, dot(high_w, spread), 0.0).astype(BF16)
        pick[1] = jnp.where(chosen, dot(low_w, spread), 0.0).astype(BF16)

    def kv_rest(s):
        x_from = (my_x + xs - s) % xs
        each(0, zs, lambda t: kv_copy(((my_z + t) % zs) * xs + x_from, me).wait_recv())

    def m_copy(q, src):
        block = xh.at[2 * q + core, rows(src, cp)]
        return send(block, block, m_s.at[q, src], m_r.at[q, src], t=mate)

    def m_arrive(q, src):
        block = xh.at[2 * q + other, rows(src, cp)]
        return send(block, block, m_s.at[q, src], m_r.at[q, src], t=mate)

    def g_copy(by, q, src):
        block = xh.at[2 * by + core, rows(src, cp)]
        return send(block, block, g_s.at[q, src], g_r.at[by, src], t=2 * q + core)

    def near_src(s):
        return near * hn + (me + hn - s) % hn

    def far_src(s):
        return far * hn + (me + hn - s) % hn

    def near_pass(s):
        src = near_src(s)

        def one(q):
            d_near(q, src, me).wait_recv()
            m_copy(q, src).start()

        each(0, ny, one)

    def far_pass(s):
        src = far_src(s)
        with jax.named_scope("fp"):
            d_far(src, me).wait_recv()
        each(1, ny, lambda t: g_copy(y, (y + t) % ny, src).start())
        m_copy(y, src).start()

    def far_pass_y(s):
        src = far_src(s)

        def one(t):
            q = (y + t) % ny
            with jax.named_scope("fpy"):
                g_copy(q, y, src).wait_recv()
            m_copy(q, src).start()

        each(1, ny, one)

    def ow_pass():
        def one(s):
            by = (y + s) % ny
            o_arrive(by).wait_recv()
            each(1, xs, lambda t: ox_copy(by, (my_x + t) % xs).start())

        each(1, ny, one)

    def ow_last():
        def one(s):
            by = (y + s) % ny
            each(1, xs, lambda t: ox_arrive(by, (my_x + t) % xs).wait_recv())
            om_copy(by, core).start()

        each(1, ny, one)

    total = kv.shape[0]
    bq = query_block(ra, total)
    per_head = ra // bq

    def attend(head, i):
        block = qs[rows(head * per_head + i, bq), :]
        scores = lax.dot_general(block, kv[...], (((1,), (1,)), ((), ())), preferred_element_type=F32)
        peak = jnp.max(scores, axis=1, keepdims=True)
        exponent = jnp.exp(scores - peak)
        row_total = jnp.sum(exponent, axis=1, keepdims=True)
        return dot(exponent.astype(BF16), kv[...]) / row_total

    def attend_pair(p, b):
        first = attend(2 * p, b)
        if heads > 1:
            both = jnp.where(left, pltpu.roll(first, HEAD_DIM, 1), attend(2 * p + 1, b))
            attf[tp, rows(b, bq), rows(p, 128)] = both.astype(BF16)
        else:
            attf[tp, rows(b, bq), :] = first[:, HEAD_DIM:].astype(BF16)

    def att_chunk(j, b):
        return attf.at[j, rows(b, bq)]

    def a_copy(by, q, b):
        return send(
            att_chunk(2 * by + core, b), att_chunk(2 * by + core, b), a_s.at[q, b], a_r.at[by, b], t=2 * q + core)

    def am_copy(by, side, b):
        return send(att_chunk(2 * by + side, b), att_chunk(2 * by + side, b), am_s.at[by, b], am_r.at[by, b], t=mate)

    def att_pass(b):
        def one(s):
            by = (y + s) % ny
            a_copy(by, y, b).wait_recv()
            am_copy(by, core, b).start()

        each(1, ny, one)

    def attend_block(b):
        each(0, pairs, lambda p: attend_pair(p, b))
        each(1, ny, lambda s: a_copy(y, (y + s) % ny, b).start())
        am_copy(y, core, b).start()
        each(b * hn // per_head, (b + 1) * hn // per_head, lambda s: finish_send(far_peer(s)))
        each(jnp.maximum(b - 1, 0), b, att_pass)

    ft = min(256, hid.shape[1])

    def gate_up(hf, t):
        at = pl.ds(pl.multiple_of(t * ft, ft), ft)
        gate = dot(xh[0, rows(hf, hs), :], wg[0:lc, at])
        up = dot(xh[0, rows(hf, hs), :], wu[0:lc, at])
        for j in range(1, tp_n):
            gate = gate + dot(xh[j, rows(hf, hs), :], wg[j * lc:(j + 1) * lc, at])
            up = up + dot(xh[j, rows(hf, hs), :], wu[j * lc:(j + 1) * lc, at])
        hid[rows(hf, hs), at] = (silu(gate) * up).astype(BF16)

    def p_copy(hf, q):
        return send(po.at[q, rows(hf, hs)], rp.at[q, rows(hf, hs)], p_s.at[hf, q], p_r.at[hf, q], t=mate)

    def down_other(hf, q):
        po[q, rows(hf, hs), :] = dot(hid[rows(hf, hs), :], wd[:, cols(2 * q + other)]).astype(BF16)
        p_copy(hf, q).start()

    def u_copy(by, q, to):
        return send(tt.at[q, rows(to, cp)], yr.at[by, rows(to, cp)], u_s.at[q, to], u_r.at[by, to], t=2 * q + core)

    def down_own(hf, q):
        own = dot(hid[rows(hf, hs), :], wd[:, cols(2 * q + core)]).astype(BF16).astype(F32)
        p_copy(hf, q).wait_recv()
        tt[q, rows(hf, hs), :] = (own + rp[q, rows(hf, hs), :].astype(F32)).astype(BF16)

    def down_away(hf, s):
        q = (y + s) % ny
        down_own(hf, q)
        each(0, hn, lambda t: u_copy(y, q, hf * hn + (me + t) % hn).start())

    def r_copy(src, to):
        return send(fin.at[rows(to, cp)], ret.at[rows(src, cp)], r_s.at[to], r_r.at[src], ep=to)

    def finish(to):
        value = tt[y, rows(to, cp), :].astype(F32)
        for t in range(1, ny):
            q = (y + t) % ny
            u_copy(q, y, to).wait_recv()
            value = value + yr[q, rows(to, cp), :].astype(F32)
        return value.astype(BF16)

    def finish_send(to):
        fin[rows(to, cp), :] = finish(to)
        r_copy(me, to).start()

    def near_wait(s):
        each(0, ny, lambda q: m_arrive(q, near_src(s)).wait_recv())

    def far_wait(s):
        each(0, ny, lambda q: m_arrive(q, far_src(s)).wait_recv())

    tiles = hid.shape[1] // ft

    def arrive(s):
        far_pass(s)
        each(s, jnp.minimum(s + 1, hn - 1), lambda t: near_pass(t + 1))

    def near_tile(t):
        gate_up(near, t)
        each(t * hn // tiles, (t + 1) * hn // tiles, far_pass_y)

    def far_tile(t):
        gate_up(far, t)
        each(1 + t * (zs - 1) // tiles, 1 + (t + 1) * (zs - 1) // tiles, kv_pass)

    with jax.named_scope("arrive"):
        each(0, hn, arrive)
    each(1, ny, lambda s: v_copy(y, (y + s) % ny).start())
    each(1, zs, lambda s: kv_copy(me, z_peer(s)).start())
    each(1, xs, lambda s: kv_copy(me, x_peer(s)).start())
    with jax.named_scope("near_wait"):
        weights[4].wait()
        weights[5].wait()
        each(1, hn, near_wait)
    with jax.named_scope("near_gate_up"):
        each(0, tiles, near_tile)
    with jax.named_scope("near_down"):
        weights[6].wait()
        each(1, ny + 1, lambda s: down_other(near, (y + s) % ny))
    with jax.named_scope("near_down_own"):
        each(1, ny, lambda s: down_away(near, s))
        down_own(near, y)
    with jax.named_scope("far_wait"):
        each(0, hn, far_wait)
    with jax.named_scope("far_gate_up"):
        each(0, tiles, far_tile)
    with jax.named_scope("ow_pass"):
        ow_pass()
    with jax.named_scope("far_down"):
        each(1, ny + 1, lambda s: down_other(far, (y + s) % ny))
        each(1, ny, lambda s: down_away(far, s))
        down_own(far, y)
    with jax.named_scope("kv_rest"):
        each(1, xs, kv_rest)
    with jax.named_scope("attend"):
        each(0, per_head, attend_block)
    with jax.named_scope("finish_near"):
        each(1, hn, lambda s: finish_send(near_peer(s)))
        ret[rows(me, cp), :] = finish(me)
    with jax.named_scope("att_wait"):
        att_pass(per_head - 1)
    with jax.named_scope("ow_last"):
        ow_last()

    with jax.named_scope("mixer"):
        each(0, ny, lambda by: each(0, per_head, lambda b: am_copy(by, other, b).wait_recv()))
        each(0, ny, lambda by: om_copy(by, other).wait_recv())
        width = mix.shape[1]
        tile = min(512, width)

        def project(t, ssq):
            at = pl.ds(pl.multiple_of(t * tile, tile), tile)
            part = dot(attf[0], ow[0:hr, at])
            for j in range(1, tp_n):
                part = part + dot(attf[j], ow[j * hr:(j + 1) * hr, at])
            mix[:, at] = part
            return ssq + jnp.sum(part * part, axis=1, keepdims=True)

        ssq = lax.fori_loop(0, width // tile, project, jnp.zeros((ra, 1), F32))
        scale = lax.rsqrt(ssq * (1.0 / width) + EPSILON)
        mixer_ref[...] = (mix[...] * scale * gain_ref[...]).astype(BF16)

    shared = shs[y].astype(F32) + shr[y].astype(F32)
    for t in range(1, ny):
        q = (y + t) % ny
        v_copy(q, y).wait_recv()
        shared = shared + shv[q].astype(F32)
    with jax.named_scope("ret_wait"):
        each(1, n, lambda s: r_copy((me + n - s) % n, me).wait_recv())
    expert_ref[...] = (dot(pick[0], ret[...]) + dot(pick[1], ret[...]) + shared).astype(BF16)

    def drain(s):
        to = (me + s) % n
        r_copy(me, to).wait_send()
        each(0, ny, lambda q: m_copy(q, to).wait_send())
        each(1, ny, lambda t: u_copy(y, (y + t) % ny, to).wait_send())

    def drain_far(s):
        d_far(me, far_peer(s)).wait_send()
        each(1, ny, lambda t: g_copy(y, (y + t) % ny, far_peer(s)).wait_send())

    def drain_y(s):
        q = (y + s) % ny
        o_copy(q).wait_send()
        each(1, xs, lambda t: ox_copy(q, (my_x + t) % xs).wait_send())
        each(0, per_head, lambda b: a_copy(y, q, b).wait_send())
        v_copy(y, q).wait_send()
        u_copy(y, q, me).wait_send()

    with jax.named_scope("drain"):
        each(1, n, drain)
        each(0, hn, drain_far)
        each(1, hn, lambda s: each(0, ny, lambda q: d_near(q, me, near_peer(s)).wait_send()))
        each(1, zs, lambda s: kv_copy(me, z_peer(s)).wait_send())
        each(1, xs, lambda s: kv_copy(me, x_peer(s)).wait_send())
        each(1, zs, lambda s: each(1, xs, lambda t: kv_forward((my_z + zs - s) % zs, t).wait_send()))
        sh_copy.wait_send()
        each(0, ny, lambda q: each(0, 2, lambda hf: p_copy(hf, q).wait_send()))
        each(0, ny, lambda by: om_copy(by, core).wait_send())
        each(0, ny, lambda by: each(0, per_head, lambda b: am_copy(by, core, b).wait_send()))
        each(1, ny, drain_y)


def store_kernel(mixed_ref, expert_ref, mixed_out, expert_out, sems):
    first = pltpu.make_async_copy(mixed_ref, mixed_out, sems.at[0])
    second = pltpu.make_async_copy(expert_ref, expert_out, sems.at[1])
    first.start()
    second.start()
    first.wait()
    second.wait()


def body(
    query_rows, key_rows, value_rows, query_gain, key_gain, out_weight, mixer_gain,
    expert_input, expert_ids, gate_score, expert_gain,
    gate_weight, up_weight, down_weight, shared_gate, shared_up, shared_down,
):
    n = lax.axis_size("ep")
    tp_n = lax.axis_size("tp")
    ny = tp_n // 2
    ra = query_rows.shape[0]
    heads = query_rows.shape[1] // HEAD_DIM
    width = out_weight.shape[1]
    rb, top = expert_ids.shape
    experts = n * gate_weight.shape[0]
    cap = 3 * rb * top // (2 * experts)
    cp = -(-cap // 16) * 16
    model = expert_input.shape[1]
    lc = model // tp_n
    xs = 1
    while 4 * xs * xs <= n:
        xs *= 2
    if heads % 2:
        query_rows = jnp.pad(query_rows, ((0, 0), (0, HEAD_DIM)))
    pairs = -(-heads // 2)
    table = jnp.asarray(position_tables(n * ra // GRID_W))

    slots = n * cp
    hidden = gate_weight.shape[2]
    sh = shared_gate.shape[1]
    hr = heads * HEAD_DIM
    blocks = ra // query_block(ra, n * ra)
    vm = pltpu.VMEM
    dma = pltpu.SemaphoreType.DMA
    vspec = pl.BlockSpec(memory_space=pltpu.VMEM)
    hspec = pl.BlockSpec(memory_space=pl.ANY)
    sizes = (n, tp_n, ny, heads, cp, lc, xs)
    mixed, expert = pl.pallas_call(
        functools.partial(fused_kernel, sizes),
        out_shape=(pltpu.VMEM((ra, width), BF16), pltpu.VMEM((rb, lc), BF16)),
        in_specs=[vspec] * 11 + [hspec] * 7,
        out_specs=(vspec, vspec),
        scratch_shapes=[
            vm((model, sh), BF16), vm((model, sh), BF16), vm((sh, model), BF16),
            vm((tp_n * hr, width), BF16),
            vm((model, hidden), BF16), vm((model, hidden), BF16), vm((hidden, model), BF16),
            vm((ra, 2 * HEAD_DIM), BF16), vm((n * ra, 2 * HEAD_DIM), BF16), vm((2 * pairs * ra, 2 * HEAD_DIM), BF16),
            vm((ra, 2 * HEAD_DIM), F32), vm((ra, 2 * HEAD_DIM), F32),
            vm((tp_n, ra, hr), BF16), vm((ra, width), F32),
            vm((rb, model), BF16), vm((slots, rb), BF16), vm((2, rb, slots), BF16),
            vm((slots // 2, lc), BF16), vm((ny, slots // 2, lc), BF16),
            vm((tp_n, slots, lc), BF16), vm((slots, hidden), BF16),
            vm((ny, slots, lc), BF16), vm((ny, slots, lc), BF16),
            vm((ny, slots, lc), BF16), vm((ny, slots, lc), BF16),
            vm((slots, lc), BF16), vm((slots, lc), BF16),
            vm((ny, rb, lc), BF16), vm((ny, rb, lc), BF16), vm((ny, rb, lc), BF16),
            vm((ny, rb, lc), BF16), vm((ny, rb, lc), BF16),
            dma((7,)), dma((n,)), dma((n,)), dma((n,)), dma((ny, n)), dma((ny, n)),
            dma((ny, n)), dma((ny, n)), dma((ny, n)), dma((ny, n)), dma((2,)), dma((ny,)), dma((ny,)),
            dma((ny,)), dma((ny,)), dma((ny, xs)), dma((ny, xs)), dma((ny,)), dma((ny,)),
            dma((ny, blocks)), dma((ny, blocks)), dma((ny, blocks)), dma((ny, blocks)),
            dma((2, ny)), dma((2, ny)), dma((ny, n)), dma((ny, n)), dma((n,)), dma((n,)),
        ],
        compiler_params=pltpu.CompilerParams(
            collective_id=0, has_side_effects=True, vmem_limit_bytes=56 * 1024 * 1024
        ),
        name="fused_layer",
    )(
        query_rows, key_rows, value_rows, query_gain.reshape(1, HEAD_DIM), key_gain.reshape(1, HEAD_DIM), table, mixer_gain.reshape(1, width),
        expert_input, expert_ids.T, gate_score.T, expert_gain.reshape(1, model),
        shared_gate, shared_up, shared_down, out_weight,
        gate_weight[0], up_weight[0], down_weight[0],
    )
    return pl.pallas_call(
        store_kernel,
        out_shape=(
            jax.ShapeDtypeStruct((ra, width), BF16),
            jax.ShapeDtypeStruct((rb, lc), BF16),
        ),
        in_specs=[vspec, vspec],
        out_specs=(hspec, hspec),
        scratch_shapes=[dma((2,))],
        name="store",
    )(pltpu.with_memory_space_constraint(mixed, pltpu.VMEM), pltpu.with_memory_space_constraint(expert, pltpu.VMEM))


def solution(mesh):
    in_specs = (
        P("ep", "tp"), P("ep", None), P("ep", None), P(), P(), P("tp", None), P(),
        P("ep", None), P("ep", None), P("ep", None), P(),
        P("ep", None, "tp"), P("ep", None, "tp"), P("ep", "tp", None),
        P(None, "tp"), P(None, "tp"), P("tp", None),
    )
    out_specs = (P("ep", None), P("ep", "tp"))
    return jax.shard_map(body, mesh=mesh, in_specs=in_specs, out_specs=out_specs, check_vma=False)
```

```python
import functools

import jax
import jax.numpy as jnp
import numpy as np
from jax import lax
from jax.experimental import pallas as pl
from jax.experimental.pallas import tpu as pltpu
from jax.sharding import PartitionSpec as P

HEADS = 16
KV_HEADS = 4
HEAD_DIM = 64
GRID_W = 64

EPSILON = 1e-06
ROUTED_SCALE = 2.5
F32 = jnp.float32
BF16 = jnp.bfloat16
MESH = pl.DeviceIdType.MESH


def position_tables(grid_rows):
    quarter = HEAD_DIM // 4
    inverse = (10000.0 ** (-np.arange(quarter, dtype=np.float32) / np.float32(quarter))).astype(np.float32)
    lane = np.arange(2 * HEAD_DIM) % (2 * quarter)
    by_row = lane < quarter
    freq = inverse[lane % quarter]
    sign = np.where(np.arange(2 * HEAD_DIM) % HEAD_DIM < HEAD_DIM // 2, -1.0, 1.0).astype(np.float32)

    def pair(count, used):
        angle = np.arange(count, dtype=np.float32)[:, None] * freq
        return [np.where(used, np.cos(angle), 0.0), np.where(used, np.sin(angle) * sign, 0.0)]

    return np.concatenate(pair(GRID_W, ~by_row) + pair(grid_rows, by_row)).astype(np.float32)


def query_block(ra, total):
    bq = max(16, min(ra, 192 * 3072 // total // 16 * 16))
    while ra % bq:
        bq -= 16
    return bq


def silu(v):
    return v / (1.0 + jnp.exp(-v))


def dot(a, b):
    return jnp.dot(a, b, preferred_element_type=F32)


def fused_kernel(
    sizes,
    q_ref, k_ref, v_ref, qg_ref, kg_ref, table_ref, gain_ref, x_ref, ids_ref, score_ref, xgain_ref,
    sg_hbm, su_hbm, sd_hbm, ow_hbm, wg_hbm, wu_hbm, wd_hbm,
    mixer_ref, expert_ref,
    sg, su, sd, ow, wg, wu, wd,
    kvo, kv, qs, cosv, sinv, attf, mix, nrm, cht, pick, outf, outn,
    xh, hid, po, rp, tt, yr, fin, ret, sho, shs, shr, shp, shv,
    w_sem, kv_s, kv_r, kf_s, d_s, d_r, m_s, m_r, g_s, g_r, sh_sem, v_s, v_r,
    o_s, o_r, ox_s, ox_r, om_s, om_r, a_s, a_r, am_s, am_r,
    p_s, p_r, u_s, u_r, r_s, r_r,
):
    n, tp_n, ny, heads, cp, lc, xs = sizes
    zs = n // xs
    hn = n // 2
    hs = hn * cp
    me = lax.axis_index("ep")
    tp = lax.axis_index("tp")
    core = tp % 2
    y = tp // 2
    mate = tp + 1 - 2 * core
    other = 1 - core
    my_z = me // xs
    my_x = me % xs
    near = me // hn
    far = 1 - near
    ra = k_ref.shape[0]
    rb, model = x_ref.shape
    slots = n * cp
    hr = ow_hbm.shape[0]
    pr = hr // xs
    pairs = -(-heads // 2)

    def send(src, dst, ssem, rsem, ep=None, t=None):
        return pltpu.make_async_remote_copy(
            src_ref=src, dst_ref=dst, send_sem=ssem, recv_sem=rsem,
            device_id=(me if ep is None else ep, tp if t is None else t), device_id_type=MESH,
        )

    def rows(block, size):
        return pl.ds(pl.multiple_of(block * size, size), size)

    def cols(tile):
        return pl.ds(pl.multiple_of(tile * lc, lc), lc)

    def each(lo, hi, fn):
        def step(i, c):
            fn(i)
            return c
        lax.fori_loop(lo, hi, step, 0)

    weights = [
        pltpu.make_async_copy(a, b, w_sem.at[i])
        for i, (a, b) in enumerate((
            (sg_hbm, sg), (su_hbm, su), (sd_hbm, sd), (ow_hbm, ow.at[rows(tp, hr)]),
            (wg_hbm, wg), (wu_hbm, wu), (wd_hbm, wd)))
    ]
    for copy in weights:
        copy.start()

    barrier = pltpu.get_barrier_semaphore()

    def greet(s):
        pl.semaphore_signal(barrier, inc=1, device_id=((me + s) % n, tp), device_id_type=MESH)

    def greet_y(s):
        pl.semaphore_signal(barrier, inc=1, device_id=(me, (tp + 2 * s) % tp_n), device_id_type=MESH)

    each(1, n, greet)
    each(1, ny, greet_y)
    pl.semaphore_signal(barrier, inc=1, device_id=(me, mate), device_id_type=MESH)

    def kv_copy(src, to):
        return send(kvo, kv.at[rows(src, ra)], kv_s.at[to], kv_r.at[src], ep=to)

    def kv_forward(src_z, s):
        src = src_z * xs + my_x
        x_to = (my_x + s) % xs
        return send(
            kv.at[rows(src, ra)], kv.at[rows(src, ra)], kf_s.at[src_z * xs + x_to], kv_r.at[src], ep=my_z * xs + x_to)

    def z_peer(s):
        return ((my_z + s) % zs) * xs + my_x

    def x_peer(s):
        return my_z * xs + (my_x + s) % xs

    def o_copy(q):
        return send(
            ow_hbm.at[rows(my_x, pr)], ow.at[pl.ds(pl.multiple_of(tp * hr + my_x * pr, pr), pr)],
            o_s.at[q], o_r.at[y], t=2 * q + core)

    def piece(by, x):
        return ow.at[pl.ds(pl.multiple_of((2 * by + core) * hr + x * pr, pr), pr)]

    def o_arrive(by):
        return send(piece(by, my_x), piece(by, my_x), o_s.at[by], o_r.at[by], t=2 * by + core)

    def ox_copy(by, x_to):
        return send(piece(by, my_x), piece(by, my_x), ox_s.at[by, x_to], ox_r.at[by, my_x], ep=my_z * xs + x_to)

    def ox_arrive(by, x_from):
        return send(
            piece(by, x_from), piece(by, x_from), ox_s.at[by, x_from], ox_r.at[by, x_from], ep=my_z * xs + x_from)

    def om_copy(by, side):
        tile = ow.at[rows(2 * by + side, hr)]
        return send(tile, tile, om_s.at[by], om_r.at[by], t=mate)

    with jax.named_scope("barrier"):
        pl.semaphore_wait(barrier, n - 1 + ny - 1 + 1)

    each(1, ny, lambda s: o_copy((y + s) % ny).start())

    x = x_ref[...].astype(F32)
    x_scale = lax.rsqrt(jnp.mean(x * x, axis=1, keepdims=True) + EPSILON)
    nrm[...] = (x * x_scale * xgain_ref[...]).astype(BF16)
    erow = lax.broadcasted_iota(jnp.int32, (128, rb), 0)
    top = ids_ref.shape[0]
    named = [ids_ref[k:k + 1, :] == erow for k in range(top)]
    member = named[0]
    for k in range(1, top):
        member = member | named[k]
    earlier = lax.broadcasted_iota(jnp.int32, (rb, rb), 0) < lax.broadcasted_iota(jnp.int32, (rb, rb), 1)
    rank = dot(jnp.where(member, 1.0, 0.0).astype(BF16), jnp.where(earlier, 1.0, 0.0).astype(BF16))
    slot_t = jnp.where(member, rank, -1.0)
    place = lax.broadcasted_iota(jnp.int32, (cp, rb), 0).astype(F32)
    for e in range(n):
        cht[e * cp:(e + 1) * cp, :] = jnp.where(slot_t[e:e + 1, :] == place, 1.0, 0.0).astype(BF16)

    def d_near(q, src, to):
        return send(
            outn.at[q, rows(to % hn, cp)], xh.at[2 * q + core, rows(src, cp)], d_s.at[q, to], d_r.at[q, src], ep=to)

    def d_far(src, to):
        return send(outf.at[rows(to % hn, cp)], xh.at[tp, rows(src, cp)], d_s.at[y, to], d_r.at[y, src], ep=to)

    def near_peer(s):
        return near * hn + (me + s) % hn

    def far_peer(s):
        return far * hn + (me + s) % hn

    for q in range(ny):
        outn[q] = dot(cht[rows(near, hs), :], nrm[:, cols(2 * q + core)]).astype(BF16)
        each(1, hn, lambda s: d_near(q, me, near_peer(s)).start())
    outf[...] = dot(cht[rows(far, hs), :], nrm[:, cols(tp)]).astype(BF16)
    each(0, hn, lambda s: d_far(me, far_peer(s)).start())
    for j in range(tp_n):
        xh[j, rows(me, cp), :] = dot(cht[rows(me, cp), :], nrm[:, j * lc:(j + 1) * lc]).astype(BF16)

    with jax.named_scope("shared"):
        for i in range(3):
            weights[i].wait()
        normed = nrm[...]
        sh_hidden = (silu(dot(normed, sg[...])) * dot(normed, su[...])).astype(BF16)
        for q in range(ny):
            sho[q] = dot(sh_hidden, sd[:, cols(2 * q + other)]).astype(BF16)
        sh_copy = send(sho, shr, sh_sem.at[0], sh_sem.at[1], t=mate)
        sh_copy.start()
        for q in range(ny):
            shs[q] = dot(sh_hidden, sd[:, cols(2 * q + core)]).astype(BF16)

    def v_copy(by, q):
        return send(shp.at[q], shv.at[by], v_s.at[q], v_r.at[by], t=2 * q + core)

    lane = lax.broadcasted_iota(jnp.int32, (1, 2 * HEAD_DIM), 1)
    left = lane < HEAD_DIM
    front = lane % HEAD_DIM < HEAD_DIM // 2
    grid_rows = (table_ref.shape[0] - 2 * GRID_W) // 2
    for g in range(ra // GRID_W):
        at = slice(g * GRID_W, (g + 1) * GRID_W)
        line = 2 * GRID_W + me * (ra // GRID_W) + g
        cosv[at, :] = table_ref[0:GRID_W, :] + table_ref[pl.ds(line, 1), :]
        sinv[at, :] = table_ref[GRID_W:2 * GRID_W, :] + table_ref[pl.ds(line + grid_rows, 1), :]

    def rotate(v):
        swapped = jnp.where(front, pltpu.roll(v, 3 * HEAD_DIM // 2, 1), pltpu.roll(v, HEAD_DIM // 2, 1))
        return v * cosv[...] + swapped * sinv[...]

    def inverse_rms(total):
        return lax.rsqrt(total * (1.0 / HEAD_DIM) + EPSILON)

    first_kv = tp * heads // (HEADS // KV_HEADS)
    kv_at = rows(first_kv // 2, 2 * HEAD_DIM)
    odd = (jnp.zeros((1, 2 * HEAD_DIM), jnp.int32) + first_kv % 2) == 1
    k_two = k_ref[:, kv_at].astype(F32)
    v_two = v_ref[:, kv_at].astype(F32)
    k_own = jnp.where(odd, pltpu.roll(k_two, HEAD_DIM, 1), k_two)
    v_own = jnp.where(odd, v_two, pltpu.roll(v_two, HEAD_DIM, 1))
    k_sum = jnp.sum(jnp.where(left, k_own * k_own, 0.0), axis=1, keepdims=True)
    k_turned = rotate(k_own * inverse_rms(k_sum) * jnp.concatenate([kg_ref[...]] * 2, axis=1))
    kv_mine = jnp.where(left, k_turned, v_own).astype(BF16)
    kvo[...] = kv_mine
    kv[rows(me, ra), :] = kv_mine

    with jax.named_scope("queries"):
        q_gain = jnp.concatenate([qg_ref[...]] * 2, axis=1)
        for p in range(pairs):
            q_two = q_ref[:, p * 128:(p + 1) * 128].astype(F32)
            square = q_two * q_two
            low = inverse_rms(jnp.sum(jnp.where(left, square, 0.0), axis=1, keepdims=True))
            high = inverse_rms(jnp.sum(jnp.where(left, 0.0, square), axis=1, keepdims=True))
            turned = rotate(q_two * jnp.where(left, low, high) * q_gain) * HEAD_DIM ** (-0.5)
            qs[2 * p * ra:(2 * p + 1) * ra, :] = jnp.where(left, turned, 0.0).astype(BF16)
            if 2 * p + 1 < heads:
                qs[(2 * p + 1) * ra:(2 * p + 2) * ra, :] = jnp.where(
                    left, pltpu.roll(turned, HEAD_DIM, 1), 0.0).astype(BF16)

    with jax.named_scope("shared_pair"):
        sh_copy.wait_recv()
        for q in range(ny):
            shp[q] = (shs[q].astype(F32) + shr[q].astype(F32)).astype(BF16)
    weights[3].wait()
    om_copy(y, core).start()

    def kv_pass(s):
        src_z = (my_z + zs - s) % zs
        kv_copy(src_z * xs + my_x, me).wait_recv()
        each(1, xs, lambda t: kv_forward(src_z, t).start())

    with jax.named_scope("pick"):
        total_score = score_ref[0:1, :]
        for k in range(1, top):
            total_score = total_score + score_ref[k:k + 1, :]
        weight_t = jnp.zeros((128, rb), F32)
        for k in range(top):
            weight_t = weight_t + jnp.where(named[k], score_ref[k:k + 1, :] / total_score * ROUTED_SCALE, 0.0)
        row_weight = weight_t.T
        slot = slot_t.T
        high_w = row_weight.astype(BF16)
        low_w = (row_weight - high_w.astype(F32)).astype(BF16)
        slot_lane = lax.broadcasted_iota(jnp.int32, (1, slots), 1).astype(F32)
        slot_expert = jnp.floor((slot_lane + 0.5) * (1.0 / cp))
        spread = jnp.where(
            lax.broadcasted_iota(jnp.int32, (128, slots), 0).astype(F32) == slot_expert, 1.0, 0.0).astype(BF16)
        chosen = dot(slot.astype(BF16), spread) == slot_lane - slot_expert * cp
        pick[0] = jnp.where(chosen, dot(high_w, spread), 0.0).astype(BF16)
        pick[1] = jnp.where(chosen, dot(low_w, spread), 0.0).astype(BF16)

    def kv_rest(s):
        x_from = (my_x + xs - s) % xs
        each(0, zs, lambda t: kv_copy(((my_z + t) % zs) * xs + x_from, me).wait_recv())

    def m_copy(q, src):
        block = xh.at[2 * q + core, rows(src, cp)]
        return send(block, block, m_s.at[q, src], m_r.at[q, src], t=mate)

    def m_arrive(q, src):
        block = xh.at[2 * q + other, rows(src, cp)]
        return send(block, block, m_s.at[q, src], m_r.at[q, src], t=mate)

    def g_copy(by, q, src):
        block = xh.at[2 * by + core, rows(src, cp)]
        return send(block, block, g_s.at[q, src], g_r.at[by, src], t=2 * q + core)

    def near_src(s):
        return near * hn + (me + hn - s) % hn

    def far_src(s):
        return far * hn + (me + hn - s) % hn

    def near_pass(s):
        src = near_src(s)

        def one(q):
            d_near(q, src, me).wait_recv()
            m_copy(q, src).start()

        each(0, ny, one)

    def far_pass(s):
        src = far_src(s)
        with jax.named_scope("fp"):
            d_far(src, me).wait_recv()
        each(1, ny, lambda t: g_copy(y, (y + t) % ny, src).start())
        m_copy(y, src).start()

    def far_pass_y(s):
        src = far_src(s)

        def one(t):
            q = (y + t) % ny
            with jax.named_scope("fpy"):
                g_copy(q, y, src).wait_recv()
            m_copy(q, src).start()

        each(1, ny, one)

    def ow_pass():
        def one(s):
            by = (y + s) % ny
            o_arrive(by).wait_recv()
            each(1, xs, lambda t: ox_copy(by, (my_x + t) % xs).start())

        each(1, ny, one)

    def ow_last():
        def one(s):
            by = (y + s) % ny
            each(1, xs, lambda t: ox_arrive(by, (my_x + t) % xs).wait_recv())
            om_copy(by, core).start()

        each(1, ny, one)

    total = kv.shape[0]
    bq = query_block(ra, total)
    per_head = ra // bq

    def attend(head, i):
        block = qs[rows(head * per_head + i, bq), :]
        scores = lax.dot_general(block, kv[...], (((1,), (1,)), ((), ())), preferred_element_type=F32)
        peak = jnp.max(scores, axis=1, keepdims=True)
        exponent = jnp.exp(scores - peak)
        row_total = jnp.sum(exponent, axis=1, keepdims=True)
        return dot(exponent.astype(BF16), kv[...]) / row_total

    def attend_pair(p, b):
        first = attend(2 * p, b)
        if heads > 1:
            both = jnp.where(left, pltpu.roll(first, HEAD_DIM, 1), attend(2 * p + 1, b))
            attf[tp, rows(b, bq), rows(p, 128)] = both.astype(BF16)
        else:
            attf[tp, rows(b, bq), :] = first[:, HEAD_DIM:].astype(BF16)

    def att_chunk(j, b):
        return attf.at[j, rows(b, bq)]

    def a_copy(by, q, b):
        return send(
            att_chunk(2 * by + core, b), att_chunk(2 * by + core, b), a_s.at[q, b], a_r.at[by, b], t=2 * q + core)

    def am_copy(by, side, b):
        return send(att_chunk(2 * by + side, b), att_chunk(2 * by + side, b), am_s.at[by, b], am_r.at[by, b], t=mate)

    def att_pass(b):
        def one(s):
            by = (y + s) % ny
            a_copy(by, y, b).wait_recv()
            am_copy(by, core, b).start()

        each(1, ny, one)

    def attend_block(b):
        each(0, pairs, lambda p: attend_pair(p, b))
        each(1, ny, lambda s: a_copy(y, (y + s) % ny, b).start())
        am_copy(y, core, b).start()
        each(b * hn // per_head, (b + 1) * hn // per_head, lambda s: finish_send(far_peer(s)))
        each(jnp.maximum(b - 1, 0), b, att_pass)

    ft = min(256, hid.shape[1])

    def gate_up(hf, t):
        at = pl.ds(pl.multiple_of(t * ft, ft), ft)
        gate = dot(xh[0, rows(hf, hs), :], wg[0:lc, at])
        up = dot(xh[0, rows(hf, hs), :], wu[0:lc, at])
        for j in range(1, tp_n):
            gate = gate + dot(xh[j, rows(hf, hs), :], wg[j * lc:(j + 1) * lc, at])
            up = up + dot(xh[j, rows(hf, hs), :], wu[j * lc:(j + 1) * lc, at])
        hid[rows(hf, hs), at] = (silu(gate) * up).astype(BF16)

    def p_copy(hf, q):
        return send(po.at[q, rows(hf, hs)], rp.at[q, rows(hf, hs)], p_s.at[hf, q], p_r.at[hf, q], t=mate)

    def down_other(hf, q):
        po[q, rows(hf, hs), :] = dot(hid[rows(hf, hs), :], wd[:, cols(2 * q + other)]).astype(BF16)
        p_copy(hf, q).start()

    def u_copy(by, q, to):
        return send(tt.at[q, rows(to, cp)], yr.at[by, rows(to, cp)], u_s.at[q, to], u_r.at[by, to], t=2 * q + core)

    def down_own(hf, q):
        own = dot(hid[rows(hf, hs), :], wd[:, cols(2 * q + core)]).astype(BF16).astype(F32)
        p_copy(hf, q).wait_recv()
        tt[q, rows(hf, hs), :] = (own + rp[q, rows(hf, hs), :].astype(F32)).astype(BF16)

    def down_away(hf, s):
        q = (y + s) % ny
        down_own(hf, q)
        each(0, hn, lambda t: u_copy(y, q, hf * hn + (me + t) % hn).start())

    def r_copy(src, to):
        return send(fin.at[rows(to, cp)], ret.at[rows(src, cp)], r_s.at[to], r_r.at[src], ep=to)

    def finish(to):
        value = tt[y, rows(to, cp), :].astype(F32)
        for t in range(1, ny):
            q = (y + t) % ny
            u_copy(q, y, to).wait_recv()
            value = value + yr[q, rows(to, cp), :].astype(F32)
        return value.astype(BF16)

    def finish_send(to):
        fin[rows(to, cp), :] = finish(to)
        r_copy(me, to).start()

    def near_wait(s):
        each(0, ny, lambda q: m_arrive(q, near_src(s)).wait_recv())

    def far_wait(s):
        each(0, ny, lambda q: m_arrive(q, far_src(s)).wait_recv())

    tiles = hid.shape[1] // ft

    def arrive(s):
        far_pass(s)
        each(s, jnp.minimum(s + 1, hn - 1), lambda t: near_pass(t + 1))

    def near_tile(t):
        gate_up(near, t)
        each(t * hn // tiles, (t + 1) * hn // tiles, far_pass_y)

    def far_tile(t):
        gate_up(far, t)

    with jax.named_scope("arrive"):
        each(0, hn, arrive)
    each(1, zs, lambda s: kv_copy(me, z_peer(s)).start())
    each(1, xs, lambda s: kv_copy(me, x_peer(s)).start())
    with jax.named_scope("near_wait"):
        weights[4].wait()
        weights[5].wait()
        each(1, hn, near_wait)
    with jax.named_scope("near_gate_up"):
        each(0, tiles, near_tile)
    with jax.named_scope("near_down"):
        weights[6].wait()
        each(1, ny + 1, lambda s: down_other(near, (y + s) % ny))
    with jax.named_scope("near_down_own"):
        each(1, ny, lambda s: down_away(near, s))
        down_own(near, y)
    with jax.named_scope("kv_pass"):
        each(1, zs, kv_pass)
    with jax.named_scope("far_wait"):
        each(0, hn, far_wait)
    with jax.named_scope("far_gate_up"):
        each(0, tiles, far_tile)
    with jax.named_scope("far_down"):
        each(1, ny + 1, lambda s: down_other(far, (y + s) % ny))
        each(1, ny, lambda s: down_away(far, s))
        down_own(far, y)
    with jax.named_scope("kv_rest"):
        each(1, xs, kv_rest)
    with jax.named_scope("ow_pass"):
        ow_pass()
    with jax.named_scope("attend"):
        each(0, per_head, attend_block)
    each(1, ny, lambda s: v_copy(y, (y + s) % ny).start())
    with jax.named_scope("finish_near"):
        each(1, hn, lambda s: finish_send(near_peer(s)))
        ret[rows(me, cp), :] = finish(me)
    with jax.named_scope("att_wait"):
        att_pass(per_head - 1)
    with jax.named_scope("ow_last"):
        ow_last()

    with jax.named_scope("mixer"):
        each(0, ny, lambda by: each(0, per_head, lambda b: am_copy(by, other, b).wait_recv()))
        each(0, ny, lambda by: om_copy(by, other).wait_recv())
        width = mix.shape[1]
        tile = min(512, width)

        def project(t, ssq):
            at = pl.ds(pl.multiple_of(t * tile, tile), tile)
            part = dot(attf[0], ow[0:hr, at])
            for j in range(1, tp_n):
                part = part + dot(attf[j], ow[j * hr:(j + 1) * hr, at])
            mix[:, at] = part
            return ssq + jnp.sum(part * part, axis=1, keepdims=True)

        ssq = lax.fori_loop(0, width // tile, project, jnp.zeros((ra, 1), F32))
        scale = lax.rsqrt(ssq * (1.0 / width) + EPSILON)
        mixer_ref[...] = (mix[...] * scale * gain_ref[...]).astype(BF16)

    shared = shs[y].astype(F32) + shr[y].astype(F32)
    for t in range(1, ny):
        q = (y + t) % ny
        v_copy(q, y).wait_recv()
        shared = shared + shv[q].astype(F32)
    with jax.named_scope("ret_wait"):
        each(1, n, lambda s: r_copy((me + n - s) % n, me).wait_recv())
    expert_ref[...] = (dot(pick[0], ret[...]) + dot(pick[1], ret[...]) + shared).astype(BF16)

    def drain(s):
        to = (me + s) % n
        r_copy(me, to).wait_send()
        each(0, ny, lambda q: m_copy(q, to).wait_send())
        each(1, ny, lambda t: u_copy(y, (y + t) % ny, to).wait_send())

    def drain_far(s):
        d_far(me, far_peer(s)).wait_send()
        each(1, ny, lambda t: g_copy(y, (y + t) % ny, far_peer(s)).wait_send())

    def drain_y(s):
        q = (y + s) % ny
        o_copy(q).wait_send()
        each(1, xs, lambda t: ox_copy(q, (my_x + t) % xs).wait_send())
        each(0, per_head, lambda b: a_copy(y, q, b).wait_send())
        v_copy(y, q).wait_send()
        u_copy(y, q, me).wait_send()

    with jax.named_scope("drain"):
        each(1, n, drain)
        each(0, hn, drain_far)
        each(1, hn, lambda s: each(0, ny, lambda q: d_near(q, me, near_peer(s)).wait_send()))
        each(1, zs, lambda s: kv_copy(me, z_peer(s)).wait_send())
        each(1, xs, lambda s: kv_copy(me, x_peer(s)).wait_send())
        each(1, zs, lambda s: each(1, xs, lambda t: kv_forward((my_z + zs - s) % zs, t).wait_send()))
        sh_copy.wait_send()
        each(0, ny, lambda q: each(0, 2, lambda hf: p_copy(hf, q).wait_send()))
        each(0, ny, lambda by: om_copy(by, core).wait_send())
        each(0, ny, lambda by: each(0, per_head, lambda b: am_copy(by, core, b).wait_send()))
        each(1, ny, drain_y)


def store_kernel(mixed_ref, expert_ref, mixed_out, expert_out, sems):
    first = pltpu.make_async_copy(mixed_ref, mixed_out, sems.at[0])
    second = pltpu.make_async_copy(expert_ref, expert_out, sems.at[1])
    first.start()
    second.start()
    first.wait()
    second.wait()


def body(
    query_rows, key_rows, value_rows, query_gain, key_gain, out_weight, mixer_gain,
    expert_input, expert_ids, gate_score, expert_gain,
    gate_weight, up_weight, down_weight, shared_gate, shared_up, shared_down,
):
    n = lax.axis_size("ep")
    tp_n = lax.axis_size("tp")
    ny = tp_n // 2
    ra = query_rows.shape[0]
    heads = query_rows.shape[1] // HEAD_DIM
    width = out_weight.shape[1]
    rb, top = expert_ids.shape
    experts = n * gate_weight.shape[0]
    cap = 3 * rb * top // (2 * experts)
    cp = -(-cap // 16) * 16
    model = expert_input.shape[1]
    lc = model // tp_n
    xs = 1
    while 4 * xs * xs <= n:
        xs *= 2
    if heads % 2:
        query_rows = jnp.pad(query_rows, ((0, 0), (0, HEAD_DIM)))
    pairs = -(-heads // 2)
    table = jnp.asarray(position_tables(n * ra // GRID_W))

    slots = n * cp
    hidden = gate_weight.shape[2]
    sh = shared_gate.shape[1]
    hr = heads * HEAD_DIM
    blocks = ra // query_block(ra, n * ra)
    vm = pltpu.VMEM
    dma = pltpu.SemaphoreType.DMA
    vspec = pl.BlockSpec(memory_space=pltpu.VMEM)
    hspec = pl.BlockSpec(memory_space=pl.ANY)
    sizes = (n, tp_n, ny, heads, cp, lc, xs)
    mixed, expert = pl.pallas_call(
        functools.partial(fused_kernel, sizes),
        out_shape=(pltpu.VMEM((ra, width), BF16), pltpu.VMEM((rb, lc), BF16)),
        in_specs=[vspec] * 11 + [hspec] * 7,
        out_specs=(vspec, vspec),
        scratch_shapes=[
            vm((model, sh), BF16), vm((model, sh), BF16), vm((sh, model), BF16),
            vm((tp_n * hr, width), BF16),
            vm((model, hidden), BF16), vm((model, hidden), BF16), vm((hidden, model), BF16),
            vm((ra, 2 * HEAD_DIM), BF16), vm((n * ra, 2 * HEAD_DIM), BF16), vm((2 * pairs * ra, 2 * HEAD_DIM), BF16),
            vm((ra, 2 * HEAD_DIM), F32), vm((ra, 2 * HEAD_DIM), F32),
            vm((tp_n, ra, hr), BF16), vm((ra, width), F32),
            vm((rb, model), BF16), vm((slots, rb), BF16), vm((2, rb, slots), BF16),
            vm((slots // 2, lc), BF16), vm((ny, slots // 2, lc), BF16),
            vm((tp_n, slots, lc), BF16), vm((slots, hidden), BF16),
            vm((ny, slots, lc), BF16), vm((ny, slots, lc), BF16),
            vm((ny, slots, lc), BF16), vm((ny, slots, lc), BF16),
            vm((slots, lc), BF16), vm((slots, lc), BF16),
            vm((ny, rb, lc), BF16), vm((ny, rb, lc), BF16), vm((ny, rb, lc), BF16),
            vm((ny, rb, lc), BF16), vm((ny, rb, lc), BF16),
            dma((7,)), dma((n,)), dma((n,)), dma((n,)), dma((ny, n)), dma((ny, n)),
            dma((ny, n)), dma((ny, n)), dma((ny, n)), dma((ny, n)), dma((2,)), dma((ny,)), dma((ny,)),
            dma((ny,)), dma((ny,)), dma((ny, xs)), dma((ny, xs)), dma((ny,)), dma((ny,)),
            dma((ny, blocks)), dma((ny, blocks)), dma((ny, blocks)), dma((ny, blocks)),
            dma((2, ny)), dma((2, ny)), dma((ny, n)), dma((ny, n)), dma((n,)), dma((n,)),
        ],
        compiler_params=pltpu.CompilerParams(
            collective_id=0, has_side_effects=True, vmem_limit_bytes=56 * 1024 * 1024
        ),
        name="fused_layer",
    )(
        query_rows, key_rows, value_rows, query_gain.reshape(1, HEAD_DIM), key_gain.reshape(1, HEAD_DIM), table, mixer_gain.reshape(1, width),
        expert_input, expert_ids.T, gate_score.T, expert_gain.reshape(1, model),
        shared_gate, shared_up, shared_down, out_weight,
        gate_weight[0], up_weight[0], down_weight[0],
    )
    return pl.pallas_call(
        store_kernel,
        out_shape=(
            jax.ShapeDtypeStruct((ra, width), BF16),
            jax.ShapeDtypeStruct((rb, lc), BF16),
        ),
        in_specs=[vspec, vspec],
        out_specs=(hspec, hspec),
        scratch_shapes=[dma((2,))],
        name="store",
    )(pltpu.with_memory_space_constraint(mixed, pltpu.VMEM), pltpu.with_memory_space_constraint(expert, pltpu.VMEM))


def solution(mesh):
    in_specs = (
        P("ep", "tp"), P("ep", None), P("ep", None), P(), P(), P("tp", None), P(),
        P("ep", None), P("ep", None), P("ep", None), P(),
        P("ep", None, "tp"), P("ep", None, "tp"), P("ep", "tp", None),
        P(None, "tp"), P(None, "tp"), P("tp", None),
    )
    out_specs = (P("ep", None), P("ep", "tp"))
    return jax.shard_map(body, mesh=mesh, in_specs=in_specs, out_specs=out_specs, check_vma=False)
```
